32 devices in a mesh: sp: 4 (over z), dp: 8 (over y, x, core).
Axes of the slice: x: 2, y: 2, z: 4, core: 2. Of those that a mesh axis runs over, the one named last changes fastest.
Arguments:
- hidden: bfloat16 [8, 512, 2048], P('dp', 'sp'), may hold values from -6 to 6
- queries: bfloat16 [8, 512, 1024], P('dp', 'sp'), may hold values from -6 to 6
- values: bfloat16 [8, 512, 2048], P('dp', 'sp'), may hold values from -6 to 6
- key_weight: bfloat16 [2048, 1024], P('dp'), may hold values from -0.125 to 0.125
- decay_down: bfloat16 [2048, 16], replicated, may hold values from -0.125 to 0.125
- decay_up: float32 [16, 1024], replicated, may hold values from -1.5 to 1.5
- decay_bias: float32 [1024], replicated, may hold values from -1 to 8
- span_shift: bfloat16 [8, 512], P('dp', 'sp'), may hold values from -1.5 to 1.5, as said below
- norm_gain: float32 [2048], replicated, may hold values from 0.1 to 1.9
Outputs:
- attended: bfloat16 [8, 512, 2048], P('dp', 'sp')
The draws below stay inside these ranges and needn't reach their ends.
Inputs may be any that keep to these rules, and one draw needn't show every extreme that they name: `span_shift`: constant over each aligned block of 64 positions.
All inputs are finite; a program needn't handle non-finite values.
Results may differ from the reference program's by a relative error of at most 0.0073.
Values may be sent and summed in bfloat16 or wider, within the bound.
No kernel may reach another device: no remote copies, remote signals or barrier semaphores. Data moves between devices by JAX's collectives and lax.ppermute only.
A program may use at most 64 MiB of HBM per device.

```python
import jax
import jax.numpy as jnp
from jax import lax

D = 2048
HEADS = 4
DK = 256
DV = 512
RANK = 16
BLOCK = 64
KEY = 1024
VAL = 2048
LENGTH = 512
BATCH = 8


def draw_decay_bias(key, part):
    pick_key, slow_key, fast_key = jax.random.split(jax.random.fold_in(key, 11), 3)
    share = 5
    slow_pick = jax.random.randint(pick_key, (KEY,), 0, 10) < share
    slow_value = jax.random.uniform(slow_key, (KEY,), jnp.float32, 6.0, 8.0)
    fast_value = jax.random.uniform(fast_key, (KEY,), jnp.float32, -1.0, 0.5)
    return jnp.where(slow_pick, slow_value, fast_value).astype(jnp.float32)


def draw_span_shift(key, part):
    level_key, sign_key = jax.random.split(jax.random.fold_in(key, 23), 2)
    blocks = LENGTH // BLOCK
    levels = jax.random.uniform(level_key, (BATCH, blocks), jnp.float32, -1.5, 1.5)
    return jnp.repeat(levels, BLOCK, axis=1).astype(jnp.bfloat16)


def steps_of(key, shape, cuts, low, top_value):
    loudness, own = 1.0, jax.random.fold_in(key, 6)
    for dim, shards_of in cuts:
        heights = jnp.exp(jax.random.uniform(jax.random.fold_in(own, dim), (shards_of,), jnp.float32, low / len(cuts), top_value / len(cuts)))
        loudness = loudness * jnp.repeat(heights, shape[dim] // shards_of).reshape([-1 if axis == dim else 1 for axis in range(len(shape))])
    return loudness


def gaussian(own_key, shape, spread, reach, cuts=(), dtype=jnp.bfloat16):
    values = jax.random.normal(own_key, shape, jnp.float32) * spread
    if len(cuts) > 0:
        values = steps_of(own_key, shape, cuts, -0.22, 0.18) * values
    return jnp.clip(values, min=-reach, max=reach).astype(dtype)


def setup_inputs(seed: int = 0) -> dict:
    splits = jax.random.split(jax.random.key(seed), 10)
    hidden = gaussian(splits[0], (BATCH, LENGTH, D), 1.0, 6.0, ((0, 8), (1, 4)))
    queries = gaussian(splits[1], (BATCH, LENGTH, KEY), 1.0, 6.0, ((0, 8), (1, 4)))
    values = gaussian(splits[2], (BATCH, LENGTH, VAL), 1.0, 6.0, ((0, 8), (1, 4)))
    key_weight = gaussian(splits[3], (D, KEY), D ** -0.5, 0.125, ((0, 8),))
    decay_down = gaussian(splits[4], (D, RANK), D ** -0.5, 0.125)
    decay_up = gaussian(splits[5], (RANK, KEY), RANK ** -0.5, 1.5, (), jnp.float32)
    decay_bias = draw_decay_bias(jax.random.fold_in(splits[9], 71), 0)
    span_shift = draw_span_shift(jax.random.fold_in(splits[9], 71), 0)
    norm_gain = jnp.clip(1.0 + 0.18 * jax.random.normal(splits[8], (VAL,), jnp.float32), 0.1, 1.9)
    return dict(hidden=hidden, queries=queries, values=values, key_weight=key_weight, decay_down=decay_down, decay_up=decay_up, decay_bias=decay_bias, span_shift=span_shift, norm_gain=norm_gain)


decay_tau = 16.0
norm_eps = 1e-05
highest = lax.Precision.HIGHEST

def mechanism(query, keys_in, value_in, log_decay):
    length, key_width = query.shape
    value_width = value_in.shape[-1]
    blocks = length // BLOCK
    step_decay = log_decay.reshape(blocks, BLOCK, key_width)
    inclusive = jnp.cumsum(step_decay, axis=1)
    exclusive = inclusive - step_decay
    total = inclusive[:, -1, :]
    query3 = query.reshape(blocks, BLOCK, key_width)
    keys3 = keys_in.reshape(blocks, BLOCK, key_width)
    value_tensor3 = value_in.reshape(blocks, BLOCK, value_width)
    query_forward_part = (query3 * jnp.exp(inclusive)).astype(jnp.bfloat16)
    key_fwd = (keys3 * jnp.exp(-inclusive)).astype(jnp.bfloat16)
    query_reverse_part = (query3 * jnp.exp(-exclusive)).astype(jnp.bfloat16)
    key_bwd = (keys3 * jnp.exp(exclusive)).astype(jnp.bfloat16)
    key_end = (keys3 * jnp.exp(total[:, None, :] - inclusive)).astype(jnp.bfloat16)
    fwd_scores = jnp.einsum('nid,njd->nij', query_forward_part, key_fwd, preferred_element_type=jnp.float32)
    bwd_scores = jnp.einsum('nid,njd->nij', query_reverse_part, key_bwd, preferred_element_type=jnp.float32)
    row_index = lax.broadcasted_iota(jnp.int32, (BLOCK, BLOCK), 0)
    col_index = lax.broadcasted_iota(jnp.int32, (BLOCK, BLOCK), 1)
    attention_scores = jnp.where((col_index <= row_index)[None], fwd_scores, bwd_scores).astype(jnp.bfloat16)
    inner_block_term = jnp.einsum('ucy,uyh->uch', attention_scores, value_tensor3, preferred_element_type=jnp.float32)
    end_terms = jnp.einsum('njd,nje->nde', key_end, value_tensor3, preferred_element_type=jnp.float32)
    start_terms = jnp.einsum('njd,nje->nde', key_bwd, value_tensor3, preferred_element_type=jnp.float32)
    rates = jnp.exp(total)

    def forward_step(carry_state, inputs):
        rate, term = inputs
        return (rate[:, None] * carry_state + term, carry_state)

    def backward_step(carry_state, inputs):
        rate, term = inputs
        state_here = rate[:, None] * carry_state
        return (state_here + term, state_here)
    empty = jnp.zeros((key_width, value_width), jnp.float32)
    _, forward_scan_states = lax.scan(forward_step, empty, (rates, end_terms))
    _, reverse_scan_states = lax.scan(backward_step, empty, (rates, start_terms), reverse=True)
    produced_rows = jnp.einsum('tzv,tvg->tzg', query_forward_part, forward_scan_states.astype(jnp.bfloat16), preferred_element_type=jnp.float32)
    produced_rows = produced_rows + jnp.einsum('tzv,tvg->tzg', query_reverse_part, reverse_scan_states.astype(jnp.bfloat16), preferred_element_type=jnp.float32)
    return (inner_block_term + produced_rows).reshape(length, value_width).astype(jnp.bfloat16)

def head_norm(mixed, gain):
    rows = mixed.shape[0]
    grouped = mixed.astype(jnp.float32).reshape(rows, HEADS, DV)
    normed = grouped * lax.rsqrt(lax.optimization_barrier(jnp.mean(grouped * grouped, axis=-1, keepdims=True)) + norm_eps)
    return (normed * gain.reshape(HEADS, DV)[None]).reshape(rows, VAL).astype(jnp.bfloat16)

def reference(hidden, queries, values, key_weight, decay_down, decay_up, decay_bias, span_shift, norm_gain):
    token_rows = hidden.reshape(-1, D)
    keys = jnp.dot(token_rows, key_weight, preferred_element_type=jnp.float32).astype(jnp.bfloat16).reshape(BATCH, LENGTH, KEY)
    low = jnp.dot(token_rows, decay_down, preferred_element_type=jnp.float32).astype(jnp.bfloat16).reshape(BATCH, LENGTH, RANK)

    def per_sequence(inputs):
        query_seq, keys_seq, value_seq, low_seq, shift_seq = inputs
        pre = jnp.dot(low_seq.astype(jnp.float32), decay_up, precision=highest, preferred_element_type=jnp.float32)
        pre = pre + decay_bias[None, :] + shift_seq.astype(jnp.float32)[:, None]
        log_decay = jax.nn.log_sigmoid(pre) / decay_tau

        def by_head(tensor, width):
            return tensor.reshape(LENGTH, HEADS, width).transpose(1, 0, 2)
        scaled = by_head(query_seq, DK).astype(jnp.float32) * DK ** (-0.5)
        mixed = jax.vmap(mechanism)(scaled, by_head(keys_seq, DK).astype(jnp.float32), by_head(value_seq, DV), by_head(log_decay, DK))
        return head_norm(mixed.transpose(1, 0, 2).reshape(LENGTH, VAL), norm_gain)
    return lax.map(per_sequence, (queries, keys, values, low, span_shift))
```

```python
import jax
import jax.numpy as jnp
from jax import lax
from jax.experimental import pallas as pl
from jax.experimental.pallas import tpu as pltpu
from jax.sharding import PartitionSpec as P

HEADS = 4
DK = 256
DV = 512
BLOCK = 64
KEY = 1024
VAL = 2048


decay_tau = 16.0
norm_eps = 1e-05
highest = lax.Precision.HIGHEST


def mechanism(query, keys_in, value_in, log_decay):
    length, key_width = query.shape
    value_width = value_in.shape[-1]
    blocks = length // BLOCK
    step_decay = log_decay.reshape(blocks, BLOCK, key_width)
    inclusive = jnp.cumsum(step_decay, axis=1)
    exclusive = inclusive - step_decay
    total = inclusive[:, -1, :]
    query3 = query.reshape(blocks, BLOCK, key_width)
    keys3 = keys_in.reshape(blocks, BLOCK, key_width)
    value_tensor3 = value_in.reshape(blocks, BLOCK, value_width)
    query_forward_part = (query3 * jnp.exp(inclusive)).astype(jnp.bfloat16)
    key_fwd = (keys3 * jnp.exp(-inclusive)).astype(jnp.bfloat16)
    query_reverse_part = (query3 * jnp.exp(-exclusive)).astype(jnp.bfloat16)
    key_bwd = (keys3 * jnp.exp(exclusive)).astype(jnp.bfloat16)
    key_end = (keys3 * jnp.exp(total[:, None, :] - inclusive)).astype(jnp.bfloat16)
    fwd_scores = jnp.einsum(
        "nid,njd->nij", query_forward_part, key_fwd, preferred_element_type=jnp.float32
    )
    bwd_scores = jnp.einsum(
        "nid,njd->nij", query_reverse_part, key_bwd, preferred_element_type=jnp.float32
    )
    row_index = lax.broadcasted_iota(jnp.int32, (BLOCK, BLOCK), 0)
    col_index = lax.broadcasted_iota(jnp.int32, (BLOCK, BLOCK), 1)
    attention_scores = jnp.where((col_index <= row_index)[None], fwd_scores, bwd_scores).astype(
        jnp.bfloat16
    )
    inner_block_term = jnp.einsum(
        "ucy,uyh->uch", attention_scores, value_tensor3, preferred_element_type=jnp.float32
    )
    end_terms = jnp.einsum(
        "njd,nje->nde", key_end, value_tensor3, preferred_element_type=jnp.float32
    )
    start_terms = jnp.einsum(
        "njd,nje->nde", key_bwd, value_tensor3, preferred_element_type=jnp.float32
    )
    rates = jnp.exp(total)

    def forward_step(carry_state, inputs):
        rate, term = inputs
        return (rate[:, None] * carry_state + term, carry_state)

    def backward_step(carry_state, inputs):
        rate, term = inputs
        state_here = rate[:, None] * carry_state
        return (state_here + term, state_here)

    empty = jnp.zeros((key_width, value_width), jnp.float32)
    _, forward_scan_states = lax.scan(forward_step, empty, (rates, end_terms))
    _, reverse_scan_states = lax.scan(backward_step, empty, (rates, start_terms), reverse=True)
    produced_rows = jnp.einsum(
        "tzv,tvg->tzg",
        query_forward_part,
        forward_scan_states.astype(jnp.bfloat16),
        preferred_element_type=jnp.float32,
    )
    produced_rows = produced_rows + jnp.einsum(
        "tzv,tvg->tzg",
        query_reverse_part,
        reverse_scan_states.astype(jnp.bfloat16),
        preferred_element_type=jnp.float32,
    )
    return (inner_block_term + produced_rows).reshape(length, value_width).astype(jnp.bfloat16)


def general_body(
    hidden, queries, values, key_weight, decay_down, decay_up, decay_bias, span_shift, norm_gain
):
    seq_count, tok_count, model_width = hidden.shape
    group_size = lax.axis_size("sp")
    value_split = group_size // HEADS
    part_width = DV // value_split
    head_index = lax.axis_index("sp") // value_split
    token_rows = hidden.reshape(tok_count, model_width)

    def per_item(tensor, width):
        by_head = tensor.reshape(tok_count, HEADS, width).transpose(1, 0, 2)
        spread_out = jnp.broadcast_to(by_head[:, None], (HEADS, value_split, tok_count, width))
        return spread_out.reshape(group_size, tok_count, width)

    def every_item(tensor):
        return jnp.broadcast_to(tensor[None], (group_size,) + tensor.shape)

    key_sums = jnp.dot(
        token_rows,
        lax.all_gather(key_weight, "dp", axis=0, tiled=True),
        preferred_element_type=jnp.float32,
    )
    keys = key_sums.astype(jnp.bfloat16)
    head_key = lax.all_to_all(per_item(keys, DK), "sp", split_axis=0, concat_axis=1, tiled=True)[0]
    low = jnp.dot(token_rows, decay_down, preferred_element_type=jnp.float32).astype(jnp.bfloat16)
    value_items = values.reshape(tok_count, group_size, part_width).transpose(1, 0, 2)
    head_query, head_value, head_low, head_shift = (
        lax.all_to_all(
            per_item(queries.reshape(tok_count, KEY), DK),
            "sp",
            split_axis=0,
            concat_axis=1,
            tiled=True,
        ),
        lax.all_to_all(value_items, "sp", split_axis=0, concat_axis=1, tiled=True),
        lax.all_to_all(every_item(low), "sp", split_axis=0, concat_axis=1, tiled=True),
        lax.all_to_all(
            every_item(span_shift.reshape(tok_count, 1)),
            "sp",
            split_axis=0,
            concat_axis=1,
            tiled=True,
        ),
    )
    up_columns = lax.dynamic_slice_in_dim(decay_up, head_index * DK, DK, 1)
    bias_part = lax.dynamic_slice_in_dim(decay_bias, head_index * DK, DK, 0)
    pre = jnp.dot(
        head_low[0].astype(jnp.float32),
        up_columns,
        precision=highest,
        preferred_element_type=jnp.float32,
    )
    pre = pre + bias_part[None, :] + head_shift[0].astype(jnp.float32)
    log_decay = jax.nn.log_sigmoid(pre) / decay_tau
    scaled = head_query[0].astype(jnp.float32) * DK ** (-0.5)
    mixed = mechanism(scaled, head_key.astype(jnp.float32), head_value[0], log_decay)
    returned = lax.all_to_all(mixed[None], "sp", split_axis=1, concat_axis=0, tiled=True)
    grouped = returned.astype(jnp.float32).transpose(1, 0, 2).reshape(tok_count, HEADS, DV)
    normed = grouped * lax.rsqrt(jnp.mean(grouped * grouped, axis=-1, keepdims=True) + norm_eps)
    normed = normed * norm_gain.reshape(HEADS, DV)[None]
    return normed.reshape(seq_count, tok_count, VAL).astype(jnp.bfloat16)


GROUP = 4 * BLOCK
PACK = 8


def exchange(tensor, axis, flip):
    size = lax.axis_size(axis)
    return lax.ppermute(tensor, axis, [(i, i ^ flip) for i in range(size)])


def dot_nn(left, right):
    return lax.dot_general(
        left, right, (((1,), (0,)), ((), ())), preferred_element_type=jnp.float32
    )


def dot_nt(left, right):
    return lax.dot_general(
        left, right, (((1,), (1,)), ((), ())), preferred_element_type=jnp.float32
    )


def dot_tn(left, right):
    return lax.dot_general(
        left, right, (((0,), (0,)), ((), ())), preferred_element_type=jnp.float32
    )


def columns_kernel(place_ref, weight_ref, out_ref):
    out_ref[...] = weight_ref[...]


def take_columns(place, weight):
    rows = weight.shape[0]
    return pl.pallas_call(
        columns_kernel,
        grid_spec=pltpu.PrefetchScalarGridSpec(
            num_scalar_prefetch=1,
            grid=(2,),
            in_specs=[pl.BlockSpec((rows, DK), lambda i, p: (0, p[0] ^ (2 * i)))],
            out_specs=pl.BlockSpec((rows, DK), lambda i, p: (0, i)),
        ),
        out_shape=jax.ShapeDtypeStruct((rows, 2 * DK), weight.dtype),
        name="columns",
    )(place, weight)


def parcels_kernel(place_ref, hidden_ref, down_ref, query_ref, value_ref, shift_ref, *out_refs):
    tok_count = query_ref.shape[0]
    low = dot_nn(hidden_ref[...], down_ref[...])
    rank = low.shape[1]
    padded = jnp.concatenate([low, jnp.zeros((tok_count, 128 - rank), jnp.float32)], axis=1)
    low_rows = padded.T.astype(jnp.bfloat16)
    shift_rows = jnp.broadcast_to(shift_ref[...].astype(jnp.float32), (PACK, tok_count))
    for flip, out_ref in enumerate(out_refs):
        head = place_ref[0] ^ flip
        out_ref[:tok_count, :DK] = query_ref[:, pl.ds(pl.multiple_of(head * DK, DK), DK)]
        out_ref[:tok_count, DK:] = value_ref[:, pl.ds(pl.multiple_of(head * DV, DV), DV)]
        out_ref[tok_count:, :tok_count] = low_rows[:PACK]
        out_ref[tok_count:, tok_count : 2 * tok_count] = low_rows[PACK : 2 * PACK]
        out_ref[tok_count:, 2 * tok_count : 3 * tok_count] = shift_rows.astype(jnp.bfloat16)
        out_ref[tok_count:, 3 * tok_count :] = jnp.zeros(
            (PACK, DK + DV - 3 * tok_count), jnp.bfloat16
        )


def make_parcels(place, token_rows, decay_down, queries, values, shift):
    tok_count = token_rows.shape[0]
    shape = jax.ShapeDtypeStruct((tok_count + PACK, DK + DV), jnp.bfloat16)
    return pl.pallas_call(
        parcels_kernel,
        in_specs=[pl.BlockSpec(memory_space=pltpu.SMEM)]
        + [pl.BlockSpec(memory_space=pltpu.VMEM)] * 5,
        out_shape=[shape] * HEADS,
        name="parcels",
    )(place, token_rows, decay_down, queries, values, shift)


def keys_kernel(rank_ref, hidden_ref, peer_ref, *refs):
    pieces, (own_ref, send_ref) = refs[:-2], refs[-2:]
    tok_count = hidden_ref.shape[0]
    sums = jnp.zeros((2 * tok_count, 2 * DK), jnp.float32)
    for flip, piece in enumerate(pieces):
        rows = piece.shape[0]
        at = pl.multiple_of((rank_ref[0] ^ flip) * rows, rows)
        both = jnp.concatenate([hidden_ref[:, pl.ds(at, rows)], peer_ref[:, pl.ds(at, rows)]], axis=0)
        sums = sums + dot_nn(both, piece[...])
    keys = sums.astype(jnp.bfloat16)
    own_ref[...] = keys[:, :DK]
    send_ref[...] = keys[:, DK:]


def project_keys(rank, token_rows, peer_rows, pieces):
    tok_count = token_rows.shape[0]
    shape = jax.ShapeDtypeStruct((2 * tok_count, DK), jnp.bfloat16)
    return pl.pallas_call(
        keys_kernel,
        in_specs=[pl.BlockSpec(memory_space=pltpu.SMEM)]
        + [pl.BlockSpec(memory_space=pltpu.VMEM)] * (2 + len(pieces)),
        out_shape=[shape, shape],
        name="keys",
    )(rank, token_rows, peer_rows, *pieces)


def split3(tensor):
    first = tensor.astype(jnp.bfloat16)
    rest = tensor - first.astype(jnp.float32)
    second = rest.astype(jnp.bfloat16)
    third = (rest - second.astype(jnp.float32)).astype(jnp.bfloat16)
    return first, second, third


def mechanism_kernel(
    place_ref, up_ref, bias_ref, gain_ref, own_ref, got_ref, p0, p1, p2, p3, *refs
):
    outs, (query_s, value_s, key_s, low_s, mixed_s, fwd_s, bwd_s) = refs[:HEADS], refs[HEADS:]
    place = place_ref[0]
    tok_count = outs[0].shape[0]
    length = query_s.shape[0]
    rank = up_ref.shape[0]
    for flip, parcel in enumerate((p0, p1, p2, p3)):
        at = pl.ds(pl.multiple_of((place ^ flip) * tok_count, tok_count), tok_count)
        query_s[at, :] = parcel[:tok_count, :DK]
        value_s[at, :] = parcel[:tok_count, DK:]
        keys = own_ref if flip < 2 else got_ref
        key_s[at, :] = keys[pl.ds((flip % 2) * tok_count, tok_count), :]
        low = parcel[tok_count:, :tok_count].astype(jnp.float32)
        high = parcel[tok_count:, tok_count : 2 * tok_count].astype(jnp.float32)
        shift = parcel[tok_count:, 2 * tok_count : 3 * tok_count].astype(jnp.float32)
        row = lax.broadcasted_iota(jnp.int32, shift.shape, 0)
        first = jnp.where(row == 0, shift, 0.0)
        stack = jnp.concatenate([low, high] * 3 + [first, jnp.zeros_like(first)], axis=0)
        low_s[:, at] = stack.astype(jnp.bfloat16)
    ones = (lax.broadcasted_iota(jnp.int32, (rank, DK), 0) == 0).astype(jnp.float32)
    up = jnp.concatenate(
        [part.astype(jnp.float32) for part in split3(up_ref[...])] + [ones], axis=0
    ).astype(jnp.bfloat16)
    pre = dot_tn(low_s[...], up) + bias_ref[...]
    log_decay = (jnp.minimum(pre, 0.0) - jnp.log1p(jnp.exp(-jnp.abs(pre)))) * (1.0 / decay_tau)

    row = lax.broadcasted_iota(jnp.int32, (GROUP, GROUP), 0)
    col = lax.broadcasted_iota(jnp.int32, (GROUP, GROUP), 1)
    same = (row // BLOCK) == (col // BLOCK)
    lower = same & (col <= row)
    upper = same & (col > row)
    sum_up_to = jnp.where(lower, 1.0, 0.0).astype(jnp.bfloat16)
    steps = [[] for _ in range(5)]
    rates = []
    for start in range(0, length, GROUP):
        decay = log_decay[start : start + GROUP]
        inclusive = sum(dot_nn(sum_up_to, part) for part in split3(decay))
        exclusive = inclusive - decay
        by_block = inclusive.reshape(GROUP // BLOCK, BLOCK, DK)
        total = by_block[:, BLOCK - 1 :, :]
        scaled = query_s[start : start + GROUP, :].astype(jnp.float32) * DK**-0.5
        keys = key_s[start : start + GROUP, :].astype(jnp.float32)
        query_fwd = (scaled * jnp.exp(inclusive)).astype(jnp.bfloat16)
        key_fwd = (keys * jnp.exp(-inclusive)).astype(jnp.bfloat16)
        query_bwd = (scaled * jnp.exp(-exclusive)).astype(jnp.bfloat16)
        key_bwd = (keys * jnp.exp(exclusive)).astype(jnp.bfloat16)
        key_end = (keys * jnp.exp(total - by_block).reshape(GROUP, DK)).astype(jnp.bfloat16)
        scores = jnp.where(
            lower, dot_nt(query_fwd, key_fwd), jnp.where(upper, dot_nt(query_bwd, key_bwd), 0.0)
        ).astype(jnp.bfloat16)
        mixed_s[start : start + GROUP, :] = dot_nn(scores, value_s[start : start + GROUP, :])
        for block in range(GROUP // BLOCK):
            at = slice(block * BLOCK, (block + 1) * BLOCK)
            for kept, tensor in zip(steps, (query_fwd, query_bwd, key_bwd, key_end)):
                kept.append(tensor[at])
            rates.append(jnp.exp(total[block]))
    query_fwd, query_bwd, key_bwd, key_end = steps[:4]
    blocks = length // BLOCK

    def rows(block):
        return slice(block * BLOCK, (block + 1) * BLOCK)

    for block in range(1, blocks):
        term = dot_tn(value_s[rows(block - 1), :], key_end[block - 1])
        if block > 1:
            term = term + fwd_s[...] * rates[block - 1]
        fwd_s[...] = term
        mixed_s[rows(block), :] += dot_nt(query_fwd[block], term.astype(jnp.bfloat16))
        back = blocks - 1 - block
        term = dot_tn(value_s[rows(back + 1), :], key_bwd[back + 1])
        if block > 1:
            term = term + bwd_s[...]
        term = term * rates[back]
        bwd_s[...] = term
        mixed_s[rows(back), :] += dot_nt(query_bwd[back], term.astype(jnp.bfloat16))

    for flip, out_ref in enumerate(outs):
        at = pl.ds(pl.multiple_of((place ^ flip) * tok_count, tok_count), tok_count)
        mixed = mixed_s[at, :].astype(jnp.bfloat16).astype(jnp.float32)
        mean = jnp.mean(mixed * mixed, axis=-1, keepdims=True)
        out_ref[...] = (mixed * lax.rsqrt(mean + norm_eps) * gain_ref[...]).astype(jnp.bfloat16)


def mix_heads(place, decay_up, decay_bias, norm_gain, own, got, parcels):
    tok_count = parcels[0].shape[0] - PACK
    length = HEADS * tok_count
    rank = decay_up.shape[0]
    whole = lambda a: pl.BlockSpec(a.shape, lambda i, p: (0,) * a.ndim)
    out = jax.ShapeDtypeStruct((tok_count, DV), jnp.bfloat16)
    return pl.pallas_call(
        mechanism_kernel,
        grid_spec=pltpu.PrefetchScalarGridSpec(
            num_scalar_prefetch=1,
            grid=(1,),
            in_specs=[
                pl.BlockSpec((rank, DK), lambda i, p: (0, p[0])),
                pl.BlockSpec((1, DK), lambda i, p: (0, p[0])),
                pl.BlockSpec((1, DV), lambda i, p: (0, p[0])),
            ]
            + [whole(a) for a in (own, got, *parcels)],
            out_specs=[whole(out)] * HEADS,
            scratch_shapes=[
                pltpu.VMEM((length, DK), jnp.bfloat16),
                pltpu.VMEM((length, DV), jnp.bfloat16),
                pltpu.VMEM((length, DK), jnp.bfloat16),
                pltpu.VMEM((4 * rank, length), jnp.bfloat16),
                pltpu.VMEM((length, DV), jnp.float32),
                pltpu.VMEM((DV, DK), jnp.float32),
                pltpu.VMEM((DV, DK), jnp.float32),
            ],
        ),
        out_shape=[out] * HEADS,
        name="mechanism",
    )(
        place,
        decay_up,
        decay_bias.reshape(1, -1),
        norm_gain.reshape(1, -1),
        own,
        got,
        *parcels,
    )


def join_kernel(place_ref, *refs):
    out_ref = refs[-1]
    for flip, part in enumerate(refs[:-1]):
        at = pl.multiple_of((place_ref[0] ^ flip) * DV, DV)
        out_ref[:, pl.ds(at, DV)] = part[...]


def join_heads(place, parts):
    return pl.pallas_call(
        join_kernel,
        in_specs=[pl.BlockSpec(memory_space=pltpu.SMEM)]
        + [pl.BlockSpec(memory_space=pltpu.VMEM)] * len(parts),
        out_shape=jax.ShapeDtypeStruct((parts[0].shape[0], VAL), jnp.bfloat16),
        name="join",
    )(place, *parts)


def paired_body(
    hidden, queries, values, key_weight, decay_down, decay_up, decay_bias, span_shift, norm_gain
):
    seq_count, tok_count, model_width = hidden.shape
    dp_size = lax.axis_size("dp")
    place = lax.axis_index("sp").reshape(1)
    rank = lax.axis_index("dp").reshape(1)
    token_rows = hidden.reshape(tok_count, model_width)

    peer_rows = exchange(token_rows, "sp", 1)
    own_piece = take_columns(place, key_weight)
    pieces = {0: own_piece}
    for flip in range(2, dp_size, 2):
        pieces[flip] = exchange(own_piece, "dp", flip)
    parcels = make_parcels(
        place,
        token_rows,
        decay_down,
        queries.reshape(tok_count, KEY),
        values.reshape(tok_count, VAL),
        span_shift.reshape(1, tok_count),
    )
    parcels = [parcels[0]] + [exchange(parcels[flip], "sp", flip) for flip in range(1, HEADS)]
    for flip in range(0, dp_size, 2):
        pieces[flip + 1] = exchange(pieces[flip], "dp", 1)
    own, sent = project_keys(rank, token_rows, peer_rows, [pieces[i] for i in range(dp_size)])
    got = exchange(sent, "sp", 2)
    outs = mix_heads(place, decay_up, decay_bias, norm_gain, own, got, parcels)
    parts = [outs[0]] + [exchange(outs[flip], "sp", flip) for flip in range(1, HEADS)]
    return join_heads(place, parts).reshape(seq_count, tok_count, VAL)


def solution(mesh):
    in_specs = (
        P("dp", "sp", None),
        P("dp", "sp", None),
        P("dp", "sp", None),
        P("dp", None),
        P(),
        P(),
        P(),
        P("dp", "sp"),
        P(),
    )
    out_specs = P("dp", "sp", None)
    paired = mesh.shape["sp"] == HEADS and mesh.shape["dp"] % 2 == 0
    body = paired_body if paired else general_body
    return jax.shard_map(body, mesh=mesh, in_specs=in_specs, out_specs=out_specs, check_vma=False)
```

```python
import jax
import jax.numpy as jnp
from jax import lax
from jax.experimental import pallas as pl
from jax.experimental.pallas import tpu as pltpu

from jax.sharding import PartitionSpec as P

HEADS = 4
DK = 256
DV = 512
BLOCK = 64
KEY = 1024
VAL = 2048


decay_tau = 16.0
norm_eps = 1e-05
highest = lax.Precision.HIGHEST


def mechanism(query, keys_in, value_in, log_decay):
    length, key_width = query.shape
    value_width = value_in.shape[-1]
    blocks = length // BLOCK
    step_decay = log_decay.reshape(blocks, BLOCK, key_width)
    inclusive = jnp.cumsum(step_decay, axis=1)
    exclusive = inclusive - step_decay
    total = inclusive[:, -1, :]
    query3 = query.reshape(blocks, BLOCK, key_width)
    keys3 = keys_in.reshape(blocks, BLOCK, key_width)
    value_tensor3 = value_in.reshape(blocks, BLOCK, value_width)
    query_forward_part = (query3 * jnp.exp(inclusive)).astype(jnp.bfloat16)
    key_fwd = (keys3 * jnp.exp(-inclusive)).astype(jnp.bfloat16)
    query_reverse_part = (query3 * jnp.exp(-exclusive)).astype(jnp.bfloat16)
    key_bwd = (keys3 * jnp.exp(exclusive)).astype(jnp.bfloat16)
    key_end = (keys3 * jnp.exp(total[:, None, :] - inclusive)).astype(jnp.bfloat16)
    fwd_scores = jnp.einsum(
        "nid,njd->nij", query_forward_part, key_fwd, preferred_element_type=jnp.float32
    )
    bwd_scores = jnp.einsum(
        "nid,njd->nij", query_reverse_part, key_bwd, preferred_element_type=jnp.float32
    )
    row_index = lax.broadcasted_iota(jnp.int32, (BLOCK, BLOCK), 0)
    col_index = lax.broadcasted_iota(jnp.int32, (BLOCK, BLOCK), 1)
    attention_scores = jnp.where((col_index <= row_index)[None], fwd_scores, bwd_scores).astype(
        jnp.bfloat16
    )
    inner_block_term = jnp.einsum(
        "ucy,uyh->uch", attention_scores, value_tensor3, preferred_element_type=jnp.float32
    )
    end_terms = jnp.einsum(
        "njd,nje->nde", key_end, value_tensor3, preferred_element_type=jnp.float32
    )
    start_terms = jnp.einsum(
        "njd,nje->nde", key_bwd, value_tensor3, preferred_element_type=jnp.float32
    )
    rates = jnp.exp(total)

    def forward_step(carry_state, inputs):
        rate, term = inputs
        return (rate[:, None] * carry_state + term, carry_state)

    def backward_step(carry_state, inputs):
        rate, term = inputs
        state_here = rate[:, None] * carry_state
        return (state_here + term, state_here)

    empty = jnp.zeros((key_width, value_width), jnp.float32)
    _, forward_scan_states = lax.scan(forward_step, empty, (rates, end_terms))
    _, reverse_scan_states = lax.scan(backward_step, empty, (rates, start_terms), reverse=True)
    produced_rows = jnp.einsum(
        "tzv,tvg->tzg",
        query_forward_part,
        forward_scan_states.astype(jnp.bfloat16),
        preferred_element_type=jnp.float32,
    )
    produced_rows = produced_rows + jnp.einsum(
        "tzv,tvg->tzg",
        query_reverse_part,
        reverse_scan_states.astype(jnp.bfloat16),
        preferred_element_type=jnp.float32,
    )
    return (inner_block_term + produced_rows).reshape(length, value_width).astype(jnp.bfloat16)


def general_body(
    hidden, queries, values, key_weight, decay_down, decay_up, decay_bias, span_shift, norm_gain
):
    seq_count, tok_count, model_width = hidden.shape
    group_size = lax.axis_size("sp")
    value_split = group_size // HEADS
    part_width = DV // value_split
    head_index = lax.axis_index("sp") // value_split
    token_rows = hidden.reshape(tok_count, model_width)

    def per_item(tensor, width):
        by_head = tensor.reshape(tok_count, HEADS, width).transpose(1, 0, 2)
        spread_out = jnp.broadcast_to(by_head[:, None], (HEADS, value_split, tok_count, width))
        return spread_out.reshape(group_size, tok_count, width)

    def every_item(tensor):
        return jnp.broadcast_to(tensor[None], (group_size,) + tensor.shape)

    key_sums = jnp.dot(
        token_rows,
        lax.all_gather(key_weight, "dp", axis=0, tiled=True),
        preferred_element_type=jnp.float32,
    )
    keys = key_sums.astype(jnp.bfloat16)
    head_key = lax.all_to_all(per_item(keys, DK), "sp", split_axis=0, concat_axis=1, tiled=True)[0]
    low = jnp.dot(token_rows, decay_down, preferred_element_type=jnp.float32).astype(jnp.bfloat16)
    value_items = values.reshape(tok_count, group_size, part_width).transpose(1, 0, 2)
    head_query, head_value, head_low, head_shift = (
        lax.all_to_all(
            per_item(queries.reshape(tok_count, KEY), DK),
            "sp",
            split_axis=0,
            concat_axis=1,
            tiled=True,
        ),
        lax.all_to_all(value_items, "sp", split_axis=0, concat_axis=1, tiled=True),
        lax.all_to_all(every_item(low), "sp", split_axis=0, concat_axis=1, tiled=True),
        lax.all_to_all(
            every_item(span_shift.reshape(tok_count, 1)),
            "sp",
            split_axis=0,
            concat_axis=1,
            tiled=True,
        ),
    )
    up_columns = lax.dynamic_slice_in_dim(decay_up, head_index * DK, DK, 1)
    bias_part = lax.dynamic_slice_in_dim(decay_bias, head_index * DK, DK, 0)
    pre = jnp.dot(
        head_low[0].astype(jnp.float32),
        up_columns,
        precision=highest,
        preferred_element_type=jnp.float32,
    )
    pre = pre + bias_part[None, :] + head_shift[0].astype(jnp.float32)
    log_decay = jax.nn.log_sigmoid(pre) / decay_tau
    scaled = head_query[0].astype(jnp.float32) * DK ** (-0.5)
    mixed = mechanism(scaled, head_key.astype(jnp.float32), head_value[0], log_decay)
    returned = lax.all_to_all(mixed[None], "sp", split_axis=1, concat_axis=0, tiled=True)
    grouped = returned.astype(jnp.float32).transpose(1, 0, 2).reshape(tok_count, HEADS, DV)
    normed = grouped * lax.rsqrt(jnp.mean(grouped * grouped, axis=-1, keepdims=True) + norm_eps)
    normed = normed * norm_gain.reshape(HEADS, DV)[None]
    return normed.reshape(seq_count, tok_count, VAL).astype(jnp.bfloat16)


GROUP = 4 * BLOCK
PACK = 8


def room(mebibytes):
    return pltpu.CompilerParams(vmem_limit_bytes=mebibytes * 2**20)


def exchange(tensor, axis, flip):
    size = lax.axis_size(axis)
    return lax.ppermute(tensor, axis, [(i, i ^ flip) for i in range(size)])


def dot_nn(left, right):
    return lax.dot_general(
        left, right, (((1,), (0,)), ((), ())), preferred_element_type=jnp.float32
    )


def dot_nt(left, right):
    return lax.dot_general(
        left, right, (((1,), (1,)), ((), ())), preferred_element_type=jnp.float32
    )


def dot_tn(left, right):
    return lax.dot_general(
        left, right, (((0,), (0,)), ((), ())), preferred_element_type=jnp.float32
    )


def columns_kernel(place_ref, weight_ref, out_ref, sems):
    copies = []
    for half in range(2):
        at = pl.multiple_of((place_ref[0] ^ (2 * half)) * DK, DK)
        copies.append(
            pltpu.make_async_copy(
                weight_ref.at[:, pl.ds(at, DK)],
                out_ref.at[:, pl.ds(half * DK, DK)],
                sems.at[half],
            )
        )
    for copy in copies:
        copy.start()
    for copy in copies:
        copy.wait()


def take_columns(place, weight):
    rows = weight.shape[0]
    return pl.pallas_call(
        columns_kernel,
        in_specs=[pl.BlockSpec(memory_space=pltpu.SMEM), pl.BlockSpec(memory_space=pl.ANY)],
        out_specs=pl.BlockSpec(memory_space=pltpu.VMEM),
        out_shape=jax.ShapeDtypeStruct((rows, 2 * DK), weight.dtype),
        scratch_shapes=[pltpu.SemaphoreType.DMA((2,))],
        compiler_params=room(8),
        name="columns",
    )(place, weight)


def parcels_kernel(place_ref, hidden_ref, down_ref, shift_ref, query_ref, value_ref, *refs):
    out_refs, sems = refs[:HEADS], refs[HEADS]
    tok_count = query_ref.shape[0]
    copies = []
    for flip, out_ref in enumerate(out_refs):
        head = place_ref[0] ^ flip
        for which, (source, width, at) in enumerate(((query_ref, DK, 0), (value_ref, DV, DK))):
            copies.append(
                pltpu.make_async_copy(
                    source.at[:, pl.ds(pl.multiple_of(head * width, width), width)],
                    out_ref.at[pl.ds(0, tok_count), pl.ds(at, width)],
                    sems.at[flip, which],
                )
            )
    for copy in copies:
        copy.start()
    low = dot_nt(down_ref[...], hidden_ref[...]).astype(jnp.bfloat16)
    shift = jnp.broadcast_to(shift_ref[...].astype(jnp.float32), (PACK, tok_count))
    empty = jnp.zeros((PACK, DK + DV - 3 * tok_count), jnp.float32)
    low = low.astype(jnp.float32)
    tail = jnp.concatenate([low[:PACK], low[PACK:], shift, empty], axis=1).astype(jnp.bfloat16)
    for out_ref in out_refs:
        out_ref[tok_count:, :] = tail
    for copy in copies:
        copy.wait()


def make_parcels(place, token_rows, decay_down, queries, values, shift):
    tok_count = token_rows.shape[0]
    shape = jax.ShapeDtypeStruct((tok_count + PACK, DK + DV), jnp.bfloat16)
    return pl.pallas_call(
        parcels_kernel,
        in_specs=[pl.BlockSpec(memory_space=pltpu.SMEM)]
        + [pl.BlockSpec(memory_space=pltpu.VMEM)] * 3
        + [pl.BlockSpec(memory_space=pl.ANY)] * 2,
        out_specs=[pl.BlockSpec(memory_space=pltpu.VMEM)] * HEADS,
        out_shape=[shape] * HEADS,
        scratch_shapes=[pltpu.SemaphoreType.DMA((HEADS, 2))],
        compiler_params=room(8),
        name="parcels",
    )(place, token_rows, decay_down.T, shift, queries, values)


def keys_kernel(rank_ref, hidden_ref, peer_ref, *refs):
    pieces, (own_ref, send_ref) = refs[:-2], refs[-2:]
    tok_count = hidden_ref.shape[0]
    sums = jnp.zeros((2 * tok_count, 2 * DK), jnp.float32)
    for flip, piece in enumerate(pieces):
        rows = piece.shape[0]
        at = pl.multiple_of((rank_ref[0] ^ flip) * rows, rows)
        both = jnp.concatenate([hidden_ref[:, pl.ds(at, rows)], peer_ref[:, pl.ds(at, rows)]], axis=0)
        sums = sums + dot_nn(both, piece[...])
    keys = sums.astype(jnp.bfloat16)
    own_ref[...] = keys[:, :DK]
    send_ref[...] = keys[:, DK:]


def project_keys(rank, token_rows, peer_rows, pieces):
    tok_count = token_rows.shape[0]
    shape = jax.ShapeDtypeStruct((2 * tok_count, DK), jnp.bfloat16)
    return pl.pallas_call(
        keys_kernel,
        in_specs=[pl.BlockSpec(memory_space=pltpu.SMEM)]
        + [pl.BlockSpec(memory_space=pltpu.VMEM)] * (2 + len(pieces)),
        out_shape=[shape, shape],
        compiler_params=room(12),
        name="keys",
    )(rank, token_rows, peer_rows, *pieces)


def split3(tensor):
    first = tensor.astype(jnp.bfloat16)
    rest = tensor - first.astype(jnp.float32)
    second = rest.astype(jnp.bfloat16)
    third = (rest - second.astype(jnp.float32)).astype(jnp.bfloat16)
    return first, second, third


def mechanism_kernel(
    place_ref, up_ref, bias_ref, gain_ref, own_ref, got_ref, p0, p1, p2, p3, *refs
):
    outs, (query_s, value_s, key_s, low_s, mixed_s, fwd_s, bwd_s) = refs[:HEADS], refs[HEADS:]
    place = place_ref[0]
    tok_count = outs[0].shape[0]
    length = query_s.shape[0]
    rank = up_ref.shape[0]
    for flip, parcel in enumerate((p0, p1, p2, p3)):
        at = pl.ds(pl.multiple_of((place ^ flip) * tok_count, tok_count), tok_count)
        query_s[at, :] = parcel[:tok_count, :DK]
        value_s[at, :] = parcel[:tok_count, DK:]
        keys = own_ref if flip < 2 else got_ref
        key_s[at, :] = keys[pl.ds((flip % 2) * tok_count, tok_count), :]
        low = parcel[tok_count:, :tok_count].astype(jnp.float32)
        high = parcel[tok_count:, tok_count : 2 * tok_count].astype(jnp.float32)
        shift = parcel[tok_count:, 2 * tok_count : 3 * tok_count].astype(jnp.float32)
        row = lax.broadcasted_iota(jnp.int32, shift.shape, 0)
        first = jnp.where(row == 0, shift, 0.0)
        stack = jnp.concatenate([low, high] * 3 + [first, jnp.zeros_like(first)], axis=0)
        low_s[:, at] = stack.astype(jnp.bfloat16)
    ones = (lax.broadcasted_iota(jnp.int32, (rank, DK), 0) == 0).astype(jnp.float32)
    up = jnp.concatenate(
        [part.astype(jnp.float32) for part in split3(up_ref[...])] + [ones], axis=0
    ).astype(jnp.bfloat16)
    pre = dot_tn(low_s[...], up) + bias_ref[...]
    log_decay = (jnp.minimum(pre, 0.0) - jnp.log1p(jnp.exp(-jnp.abs(pre)))) * (1.0 / decay_tau)

    row = lax.broadcasted_iota(jnp.int32, (GROUP, GROUP), 0)
    col = lax.broadcasted_iota(jnp.int32, (GROUP, GROUP), 1)
    same = (row // BLOCK) == (col // BLOCK)
    lower = same & (col <= row)
    upper = same & (col > row)
    sum_up_to = jnp.where(lower, 1.0, 0.0).astype(jnp.bfloat16)
    steps = [[] for _ in range(5)]
    rates = []
    for start in range(0, length, GROUP):
        decay = log_decay[start : start + GROUP]
        inclusive = sum(dot_nn(sum_up_to, part) for part in split3(decay))
        exclusive = inclusive - decay
        by_block = inclusive.reshape(GROUP // BLOCK, BLOCK, DK)
        total = by_block[:, BLOCK - 1 :, :]
        scaled = query_s[start : start + GROUP, :].astype(jnp.float32) * DK**-0.5
        keys = key_s[start : start + GROUP, :].astype(jnp.float32)
        query_fwd = (scaled * jnp.exp(inclusive)).astype(jnp.bfloat16)
        key_fwd = (keys * jnp.exp(-inclusive)).astype(jnp.bfloat16)
        query_bwd = (scaled * jnp.exp(-exclusive)).astype(jnp.bfloat16)
        key_bwd = (keys * jnp.exp(exclusive)).astype(jnp.bfloat16)
        key_end = (keys * jnp.exp(total - by_block).reshape(GROUP, DK)).astype(jnp.bfloat16)
        scores = jnp.where(
            lower, dot_nt(query_fwd, key_fwd), jnp.where(upper, dot_nt(query_bwd, key_bwd), 0.0)
        ).astype(jnp.bfloat16)
        mixed_s[start : start + GROUP, :] = dot_nn(scores, value_s[start : start + GROUP, :])
        for block in range(GROUP // BLOCK):
            at = slice(block * BLOCK, (block + 1) * BLOCK)
            for kept, tensor in zip(steps, (query_fwd, query_bwd, key_bwd, key_end)):
                kept.append(tensor[at])
            rates.append(jnp.exp(total[block]))
    query_fwd, query_bwd, key_bwd, key_end = steps[:4]
    blocks = length // BLOCK

    def rows(block):
        return slice(block * BLOCK, (block + 1) * BLOCK)

    for block in range(1, blocks):
        term = dot_tn(value_s[rows(block - 1), :], key_end[block - 1])
        if block > 1:
            term = term + fwd_s[...] * rates[block - 1]
        fwd_s[...] = term
        mixed_s[rows(block), :] += dot_nt(query_fwd[block], term.astype(jnp.bfloat16))
        back = blocks - 1 - block
        term = dot_tn(value_s[rows(back + 1), :], key_bwd[back + 1])
        if block > 1:
            term = term + bwd_s[...]
        term = term * rates[back]
        bwd_s[...] = term
        mixed_s[rows(back), :] += dot_nt(query_bwd[back], term.astype(jnp.bfloat16))

    for flip, out_ref in enumerate(outs):
        at = pl.ds(pl.multiple_of((place ^ flip) * tok_count, tok_count), tok_count)
        mixed = mixed_s[at, :].astype(jnp.bfloat16).astype(jnp.float32)
        mean = jnp.mean(mixed * mixed, axis=-1, keepdims=True)
        out_ref[...] = (mixed * lax.rsqrt(mean + norm_eps) * gain_ref[...]).astype(jnp.bfloat16)


def mix_heads(place, decay_up, decay_bias, norm_gain, own, got, parcels):
    tok_count = parcels[0].shape[0] - PACK
    length = HEADS * tok_count
    rank = decay_up.shape[0]
    whole = lambda a: pl.BlockSpec(a.shape, lambda i, p: (0,) * a.ndim)
    out = jax.ShapeDtypeStruct((tok_count, DV), jnp.bfloat16)
    return pl.pallas_call(
        mechanism_kernel,
        grid_spec=pltpu.PrefetchScalarGridSpec(
            num_scalar_prefetch=1,
            grid=(1,),
            in_specs=[
                pl.BlockSpec((rank, DK), lambda i, p: (0, p[0])),
                pl.BlockSpec((1, DK), lambda i, p: (0, p[0])),
                pl.BlockSpec((1, DV), lambda i, p: (0, p[0])),
            ]
            + [whole(a) for a in (own, got, *parcels)],
            out_specs=[whole(out)] * HEADS,
            scratch_shapes=[
                pltpu.VMEM((length, DK), jnp.bfloat16),
                pltpu.VMEM((length, DV), jnp.bfloat16),
                pltpu.VMEM((length, DK), jnp.bfloat16),
                pltpu.VMEM((4 * rank, length), jnp.bfloat16),
                pltpu.VMEM((length, DV), jnp.float32),
                pltpu.VMEM((DV, DK), jnp.float32),
                pltpu.VMEM((DV, DK), jnp.float32),
            ],
        ),
        out_shape=[out] * HEADS,
        compiler_params=room(24),
        name="mechanism",
    )(
        place,
        decay_up,
        decay_bias.reshape(1, -1),
        norm_gain.reshape(1, -1),
        own,
        got,
        *parcels,
    )


def join_kernel(place_ref, *refs):
    out_ref = refs[-1]
    for flip, part in enumerate(refs[:-1]):
        at = pl.multiple_of((place_ref[0] ^ flip) * DV, DV)
        out_ref[:, pl.ds(at, DV)] = part[...]


def join_heads(place, parts):
    return pl.pallas_call(
        join_kernel,
        in_specs=[pl.BlockSpec(memory_space=pltpu.SMEM)]
        + [pl.BlockSpec(memory_space=pltpu.VMEM)] * len(parts),
        out_shape=jax.ShapeDtypeStruct((parts[0].shape[0], VAL), jnp.bfloat16),
        compiler_params=room(8),
        name="join",
    )(place, *parts)


def paired_body(
    hidden, queries, values, key_weight, decay_down, decay_up, decay_bias, span_shift, norm_gain
):
    seq_count, tok_count, model_width = hidden.shape
    dp_size = lax.axis_size("dp")
    place = lax.axis_index("sp").reshape(1)
    rank = lax.axis_index("dp").reshape(1)
    token_rows = hidden.reshape(tok_count, model_width)

    peer_rows = exchange(token_rows, "sp", 1)
    own_piece = take_columns(place, key_weight)
    pieces = {0: own_piece}
    for flip in range(2, dp_size, 2):
        pieces[flip] = exchange(own_piece, "dp", flip)
    parcels = make_parcels(
        place,
        token_rows,
        decay_down,
        queries.reshape(tok_count, KEY),
        values.reshape(tok_count, VAL),
        span_shift.reshape(1, tok_count),
    )
    parcels = [parcels[0]] + [exchange(parcels[flip], "sp", flip) for flip in range(1, HEADS)]
    for flip in range(0, dp_size, 2):
        pieces[flip + 1] = exchange(pieces[flip], "dp", 1)
    own, sent = project_keys(rank, token_rows, peer_rows, [pieces[i] for i in range(dp_size)])
    got = exchange(sent, "sp", 2)
    outs = mix_heads(place, decay_up, decay_bias, norm_gain, own, got, parcels)
    parts = [outs[0]] + [exchange(outs[flip], "sp", flip) for flip in range(1, HEADS)]
    return join_heads(place, parts).reshape(seq_count, tok_count, VAL)


def solution(mesh):
    in_specs = (
        P("dp", "sp", None),
        P("dp", "sp", None),
        P("dp", "sp", None),
        P("dp", None),
        P(),
        P(),
        P(),
        P("dp", "sp"),
        P(),
    )
    out_specs = P("dp", "sp", None)
    paired = mesh.shape["sp"] == HEADS and mesh.shape["dp"] % 2 == 0
    body = paired_body if paired else general_body

    return jax.shard_map(body, mesh=mesh, in_specs=in_specs, out_specs=out_specs, check_vma=False)
```

```python
import jax
import jax.numpy as jnp
from jax import lax
from jax.experimental import pallas as pl
from jax.experimental.pallas import tpu as pltpu

from jax.sharding import PartitionSpec as P

HEADS = 4
DK = 256
DV = 512
BLOCK = 64
KEY = 1024
VAL = 2048


decay_tau = 16.0
norm_eps = 1e-05
highest = lax.Precision.HIGHEST


def mechanism(query, keys_in, value_in, log_decay):
    length, key_width = query.shape
    value_width = value_in.shape[-1]
    blocks = length // BLOCK
    step_decay = log_decay.reshape(blocks, BLOCK, key_width)
    inclusive = jnp.cumsum(step_decay, axis=1)
    exclusive = inclusive - step_decay
    total = inclusive[:, -1, :]
    query3 = query.reshape(blocks, BLOCK, key_width)
    keys3 = keys_in.reshape(blocks, BLOCK, key_width)
    value_tensor3 = value_in.reshape(blocks, BLOCK, value_width)
    query_forward_part = (query3 * jnp.exp(inclusive)).astype(jnp.bfloat16)
    key_fwd = (keys3 * jnp.exp(-inclusive)).astype(jnp.bfloat16)
    query_reverse_part = (query3 * jnp.exp(-exclusive)).astype(jnp.bfloat16)
    key_bwd = (keys3 * jnp.exp(exclusive)).astype(jnp.bfloat16)
    key_end = (keys3 * jnp.exp(total[:, None, :] - inclusive)).astype(jnp.bfloat16)
    fwd_scores = jnp.einsum(
        "nid,njd->nij", query_forward_part, key_fwd, preferred_element_type=jnp.float32
    )
    bwd_scores = jnp.einsum(
        "nid,njd->nij", query_reverse_part, key_bwd, preferred_element_type=jnp.float32
    )
    row_index = lax.broadcasted_iota(jnp.int32, (BLOCK, BLOCK), 0)
    col_index = lax.broadcasted_iota(jnp.int32, (BLOCK, BLOCK), 1)
    attention_scores = jnp.where((col_index <= row_index)[None], fwd_scores, bwd_scores).astype(
        jnp.bfloat16
    )
    inner_block_term = jnp.einsum(
        "ucy,uyh->uch", attention_scores, value_tensor3, preferred_element_type=jnp.float32
    )
    end_terms = jnp.einsum(
        "njd,nje->nde", key_end, value_tensor3, preferred_element_type=jnp.float32
    )
    start_terms = jnp.einsum(
        "njd,nje->nde", key_bwd, value_tensor3, preferred_element_type=jnp.float32
    )
    rates = jnp.exp(total)

    def forward_step(carry_state, inputs):
        rate, term = inputs
        return (rate[:, None] * carry_state + term, carry_state)

    def backward_step(carry_state, inputs):
        rate, term = inputs
        state_here = rate[:, None] * carry_state
        return (state_here + term, state_here)

    empty = jnp.zeros((key_width, value_width), jnp.float32)
    _, forward_scan_states = lax.scan(forward_step, empty, (rates, end_terms))
    _, reverse_scan_states = lax.scan(backward_step, empty, (rates, start_terms), reverse=True)
    produced_rows = jnp.einsum(
        "tzv,tvg->tzg",
        query_forward_part,
        forward_scan_states.astype(jnp.bfloat16),
        preferred_element_type=jnp.float32,
    )
    produced_rows = produced_rows + jnp.einsum(
        "tzv,tvg->tzg",
        query_reverse_part,
        reverse_scan_states.astype(jnp.bfloat16),
        preferred_element_type=jnp.float32,
    )
    return (inner_block_term + produced_rows).reshape(length, value_width).astype(jnp.bfloat16)


def general_body(
    hidden, queries, values, key_weight, decay_down, decay_up, decay_bias, span_shift, norm_gain
):
    seq_count, tok_count, model_width = hidden.shape
    group_size = lax.axis_size("sp")
    value_split = group_size // HEADS
    part_width = DV // value_split
    head_index = lax.axis_index("sp") // value_split
    token_rows = hidden.reshape(tok_count, model_width)

    def per_item(tensor, width):
        by_head = tensor.reshape(tok_count, HEADS, width).transpose(1, 0, 2)
        spread_out = jnp.broadcast_to(by_head[:, None], (HEADS, value_split, tok_count, width))
        return spread_out.reshape(group_size, tok_count, width)

    def every_item(tensor):
        return jnp.broadcast_to(tensor[None], (group_size,) + tensor.shape)

    key_sums = jnp.dot(
        token_rows,
        lax.all_gather(key_weight, "dp", axis=0, tiled=True),
        preferred_element_type=jnp.float32,
    )
    keys = key_sums.astype(jnp.bfloat16)
    head_key = lax.all_to_all(per_item(keys, DK), "sp", split_axis=0, concat_axis=1, tiled=True)[0]
    low = jnp.dot(token_rows, decay_down, preferred_element_type=jnp.float32).astype(jnp.bfloat16)
    value_items = values.reshape(tok_count, group_size, part_width).transpose(1, 0, 2)
    head_query, head_value, head_low, head_shift = (
        lax.all_to_all(
            per_item(queries.reshape(tok_count, KEY), DK),
            "sp",
            split_axis=0,
            concat_axis=1,
            tiled=True,
        ),
        lax.all_to_all(value_items, "sp", split_axis=0, concat_axis=1, tiled=True),
        lax.all_to_all(every_item(low), "sp", split_axis=0, concat_axis=1, tiled=True),
        lax.all_to_all(
            every_item(span_shift.reshape(tok_count, 1)),
            "sp",
            split_axis=0,
            concat_axis=1,
            tiled=True,
        ),
    )
    up_columns = lax.dynamic_slice_in_dim(decay_up, head_index * DK, DK, 1)
    bias_part = lax.dynamic_slice_in_dim(decay_bias, head_index * DK, DK, 0)
    pre = jnp.dot(
        head_low[0].astype(jnp.float32),
        up_columns,
        precision=highest,
        preferred_element_type=jnp.float32,
    )
    pre = pre + bias_part[None, :] + head_shift[0].astype(jnp.float32)
    log_decay = jax.nn.log_sigmoid(pre) / decay_tau
    scaled = head_query[0].astype(jnp.float32) * DK ** (-0.5)
    mixed = mechanism(scaled, head_key.astype(jnp.float32), head_value[0], log_decay)
    returned = lax.all_to_all(mixed[None], "sp", split_axis=1, concat_axis=0, tiled=True)
    grouped = returned.astype(jnp.float32).transpose(1, 0, 2).reshape(tok_count, HEADS, DV)
    normed = grouped * lax.rsqrt(jnp.mean(grouped * grouped, axis=-1, keepdims=True) + norm_eps)
    normed = normed * norm_gain.reshape(HEADS, DV)[None]
    return normed.reshape(seq_count, tok_count, VAL).astype(jnp.bfloat16)


PACK = 8


def room(mebibytes):
    return pltpu.CompilerParams(vmem_limit_bytes=mebibytes * 2**20)


def exchange(tensor, axis, flip):
    size = lax.axis_size(axis)
    return lax.ppermute(tensor, axis, [(i, i ^ flip) for i in range(size)])


def dot_nn(left, right):
    return lax.dot_general(
        left, right, (((1,), (0,)), ((), ())), preferred_element_type=jnp.float32
    )


def dot_nt(left, right):
    return lax.dot_general(
        left, right, (((1,), (1,)), ((), ())), preferred_element_type=jnp.float32
    )


def dot_tn(left, right):
    return lax.dot_general(
        left, right, (((0,), (0,)), ((), ())), preferred_element_type=jnp.float32
    )


def columns_kernel(place_ref, weight_ref, out_ref, sems):
    copies = []
    for half in range(2):
        at = pl.multiple_of((place_ref[0] ^ (2 * half)) * DK, DK)
        copies.append(
            pltpu.make_async_copy(
                weight_ref.at[:, pl.ds(at, DK)],
                out_ref.at[:, pl.ds(half * DK, DK)],
                sems.at[half],
            )
        )
    for copy in copies:
        copy.start()
    for copy in copies:
        copy.wait()


def take_columns(place, weight):
    rows = weight.shape[0]
    return pl.pallas_call(
        columns_kernel,
        in_specs=[pl.BlockSpec(memory_space=pltpu.SMEM), pl.BlockSpec(memory_space=pl.ANY)],
        out_specs=pl.BlockSpec(memory_space=pltpu.VMEM),
        out_shape=jax.ShapeDtypeStruct((rows, 2 * DK), weight.dtype),
        scratch_shapes=[pltpu.SemaphoreType.DMA((2,))],
        compiler_params=room(8),
        name="columns",
    )(place, pltpu.with_memory_space_constraint(weight, pltpu.HBM))


def parcels_kernel(place_ref, hidden_ref, down_ref, shift_ref, query_ref, value_ref, *refs):
    out_refs, sems = refs[:HEADS], refs[HEADS]
    tok_count = query_ref.shape[0]
    copies = []
    for flip, out_ref in enumerate(out_refs):
        head = place_ref[0] ^ flip
        for which, (source, width, at) in enumerate(((query_ref, DK, 0), (value_ref, DV, DK))):
            copies.append(
                pltpu.make_async_copy(
                    source.at[:, pl.ds(pl.multiple_of(head * width, width), width)],
                    out_ref.at[pl.ds(0, tok_count), pl.ds(at, width)],
                    sems.at[flip, which],
                )
            )
    for copy in copies:
        copy.start()
    low = dot_nt(down_ref[...], hidden_ref[...]).astype(jnp.bfloat16)
    shift = jnp.broadcast_to(shift_ref[...].astype(jnp.float32), (PACK, tok_count))
    empty = jnp.zeros((PACK, DK + DV - 3 * tok_count), jnp.float32)
    low = low.astype(jnp.float32)
    tail = jnp.concatenate([low[:PACK], low[PACK:], shift, empty], axis=1).astype(jnp.bfloat16)
    for out_ref in out_refs:
        out_ref[tok_count:, :] = tail
    for copy in copies:
        copy.wait()


def make_parcels(place, token_rows, decay_down, queries, values, shift):
    tok_count = token_rows.shape[0]
    shape = jax.ShapeDtypeStruct((tok_count + PACK, DK + DV), jnp.bfloat16)
    return pl.pallas_call(
        parcels_kernel,
        in_specs=[pl.BlockSpec(memory_space=pltpu.SMEM)]
        + [pl.BlockSpec(memory_space=pltpu.VMEM)] * 3
        + [pl.BlockSpec(memory_space=pl.ANY)] * 2,
        out_specs=[pl.BlockSpec(memory_space=pltpu.VMEM)] * HEADS,
        out_shape=[shape] * HEADS,
        scratch_shapes=[pltpu.SemaphoreType.DMA((HEADS, 2))],
        compiler_params=room(8),
        name="parcels",
    )(
        place,
        token_rows,
        decay_down.T,
        shift,
        *(pltpu.with_memory_space_constraint(a, pltpu.HBM) for a in (queries, values)),
    )


def keys_kernel(rank_ref, hidden_ref, peer_ref, *refs):
    pieces, (own_ref, send_ref) = refs[:-2], refs[-2:]
    tok_count = hidden_ref.shape[0]
    sums = jnp.zeros((2 * tok_count, 2 * DK), jnp.float32)
    for flip, piece in enumerate(pieces):
        rows = piece.shape[0]
        at = pl.multiple_of((rank_ref[0] ^ flip) * rows, rows)
        both = jnp.concatenate([hidden_ref[:, pl.ds(at, rows)], peer_ref[:, pl.ds(at, rows)]], axis=0)
        sums = sums + dot_nn(both, piece[...])
    keys = sums.astype(jnp.bfloat16)
    own_ref[...] = keys[:, :DK]
    send_ref[...] = keys[:, DK:]


def project_keys(rank, token_rows, peer_rows, pieces):
    tok_count = token_rows.shape[0]
    shape = jax.ShapeDtypeStruct((2 * tok_count, DK), jnp.bfloat16)
    return pl.pallas_call(
        keys_kernel,
        in_specs=[pl.BlockSpec(memory_space=pltpu.SMEM)]
        + [pl.BlockSpec(memory_space=pltpu.VMEM)] * (2 + len(pieces)),
        out_shape=[shape, shape],
        compiler_params=room(12),
        name="keys",
    )(rank, token_rows, peer_rows, *pieces)


def split3(tensor):
    first = tensor.astype(jnp.bfloat16)
    rest = tensor - first.astype(jnp.float32)
    second = rest.astype(jnp.bfloat16)
    third = (rest - second.astype(jnp.float32)).astype(jnp.bfloat16)
    return first, second, third


def in_blocks(tensor):
    return [tensor[at : at + BLOCK] for at in range(0, tensor.shape[0], BLOCK)]


def arrange(place, target, near, far, columns):
    tok_count = target.shape[0] // 2
    half = place & 1
    for which, part in ((half, near), (1 - half, far)):
        at = pl.ds(pl.multiple_of(which * tok_count, tok_count), tok_count)
        target[at, :] = part[:tok_count, columns]


def arrange_low(place, target, near, far):
    tok_count = target.shape[1] // 2
    half = place & 1
    for which, part in ((half, near), (1 - half, far)):
        low = part[tok_count:, :tok_count].astype(jnp.float32)
        high = part[tok_count:, tok_count : 2 * tok_count].astype(jnp.float32)
        shift = part[tok_count:, 2 * tok_count : 3 * tok_count].astype(jnp.float32)
        row = lax.broadcasted_iota(jnp.int32, shift.shape, 0)
        first = jnp.where(row == 0, shift, 0.0)
        stack = jnp.concatenate([low, high] * 3 + [first, jnp.zeros_like(first)], axis=0)
        at = pl.ds(pl.multiple_of(which * tok_count, tok_count), tok_count)
        target[:, at] = stack.astype(jnp.bfloat16)


def decay_of(low, up, bias, sum_up_to):
    pre = dot_tn(low, up) + bias
    decay = (jnp.minimum(pre, 0.0) - jnp.log1p(jnp.exp(-jnp.abs(pre)))) * (1.0 / decay_tau)
    inclusive = sum(dot_nn(sum_up_to, part) for part in split3(decay))
    return decay, inclusive


def scores_of(query_fwd, query_bwd, key_fwd, key_bwd, key_end, rates):
    blocks = len(rates)
    short = lambda tensors: [tensor.astype(jnp.bfloat16) for tensor in tensors]
    key_fwd, near_bwd = short(key_fwd), short(key_bwd)
    width = blocks * BLOCK
    row = lax.broadcasted_iota(jnp.int32, (BLOCK, width), 0)
    col = lax.broadcasted_iota(jnp.int32, (BLOCK, width), 1)
    rows = []
    for here in range(blocks):
        left, right = list(key_fwd), list(near_bwd)
        for past in range(here):
            faded = key_end[past]
            for between in range(past + 1, here):
                faded = faded * rates[between]
            left[past] = faded.astype(jnp.bfloat16)
        fade = None
        for later in range(here + 1, blocks):
            fade = rates[later - 1] if fade is None else fade * rates[later - 1]
            right[later] = (key_bwd[later] * fade).astype(jnp.bfloat16)
        fwd = dot_nt(query_fwd[here], jnp.concatenate(left, axis=0))
        bwd = dot_nt(query_bwd[here], jnp.concatenate(right, axis=0))
        rows.append(jnp.where(col <= row + here * BLOCK, fwd, bwd).astype(jnp.bfloat16))
    return jnp.concatenate(rows, axis=0)


def factors(decay, inclusive, facing_right):
    blocks = zip(in_blocks(decay), in_blocks(inclusive))
    decay, inclusive = map(list, zip(*blocks))
    totals = [tensor[BLOCK - 1 :] for tensor in inclusive]
    none = jnp.zeros_like(totals[0])
    right = jnp.where(facing_right, 1.0, 0.0)
    found = []
    for at in range(len(totals)):
        exclusive = inclusive[at] - decay[at]
        before = sum(totals[:at], none)
        after = sum(totals[at:], none)
        base = right * after + (1.0 - right) * before
        sign = 1.0 - 2.0 * right
        found.append(
            dict(
                query_fwd=jnp.exp(inclusive[at]),
                query_bwd=jnp.exp(-exclusive),
                key_fwd=jnp.exp(-inclusive[at]),
                key_bwd=jnp.exp(exclusive),
                key_end=jnp.exp(totals[at] - inclusive[at]),
                key_edge=jnp.exp(base + sign * (exclusive + right * decay[at])),
                query_edge=jnp.exp(base + sign * (inclusive[at] - right * decay[at])),
                rate=jnp.exp(totals[at]),
            )
        )
    return {name: [one[name] for one in found] for name in found[0]}


def early_kernel(place_ref, up_ref, bias_ref, own_ref, p0, p1, p2, p3, *refs):
    (
        mixed_a,
        mixed_b,
        query_edge_a,
        query_fwd_b,
        query_bwd_b,
        fwd_b,
        bwd_b,
        end_b,
        edge_b,
        rate_b,
        query_s,
        value_s,
        key_s,
        low_s,
        far_query_s,
        far_low_s,
    ) = refs
    place = place_ref[0]
    rank = up_ref.shape[0]
    size = mixed_a.shape[0]
    at = pl.ds(pl.multiple_of(place * DK, DK), DK)
    ones = (lax.broadcasted_iota(jnp.int32, (rank, DK), 0) == 0).astype(jnp.float32)
    up = jnp.concatenate(
        [part.astype(jnp.float32) for part in split3(up_ref[:, at])] + [ones], axis=0
    ).astype(jnp.bfloat16)
    bias = bias_ref[:, at]
    row = lax.broadcasted_iota(jnp.int32, (size, size), 0)
    col = lax.broadcasted_iota(jnp.int32, (size, size), 1)
    lower = ((row // BLOCK) == (col // BLOCK)) & (col <= row)
    sum_up_to = jnp.where(lower, 1.0, 0.0).astype(jnp.bfloat16)
    first_pair = place < HEADS // 2
    join = lambda tensors: jnp.concatenate(tensors, axis=0)
    times = lambda left, right: [a * b for a, b in zip(left, right)]
    short = lambda tensors: [tensor.astype(jnp.bfloat16) for tensor in tensors]

    arrange_low(place, low_s, p0, p1)
    arrange(place, query_s, p0, p1, slice(0, DK))
    arrange(place, value_s, p0, p1, slice(DK, DK + DV))
    arrange(place, key_s, own_ref.at[:size // 2], own_ref.at[size // 2 :], slice(0, DK))
    found = factors(*decay_of(low_s[...], up, bias, sum_up_to), first_pair)
    scaled = in_blocks(query_s[...].astype(jnp.float32) * DK**-0.5)
    keys = in_blocks(key_s[...].astype(jnp.float32))
    scores = scores_of(
        short(times(scaled, found["query_fwd"])),
        short(times(scaled, found["query_bwd"])),
        times(keys, found["key_fwd"]),
        times(keys, found["key_bwd"]),
        times(keys, found["key_end"]),
        found["rate"],
    )
    mixed_a[...] = dot_nn(scores, value_s[...])
    query_edge_a[...] = join(short(times(scaled, found["query_edge"])))
    key_edge = join(short(times(keys, found["key_edge"])))
    state = dot_tn(key_edge, value_s[...]).astype(jnp.bfloat16)

    arrange_low(place, far_low_s, p2, p3)
    arrange(place, far_query_s, p2, p3, slice(0, DK))
    found = factors(*decay_of(far_low_s[...], up, bias, sum_up_to), jnp.logical_not(first_pair))
    scaled = in_blocks(far_query_s[...].astype(jnp.float32) * DK**-0.5)
    query_fwd_b[...] = join(short(times(scaled, found["query_fwd"])))
    query_bwd_b[...] = join(short(times(scaled, found["query_bwd"])))
    mixed_b[...] = dot_nn(join(short(times(scaled, found["query_edge"]))), state)
    fwd_b[...] = join(found["key_fwd"])
    bwd_b[...] = join(found["key_bwd"])
    end_b[...] = join(found["key_end"])
    edge_b[...] = join(found["key_edge"])
    for at, rate in enumerate(found["rate"]):
        rate_b[at * PACK : (at + 1) * PACK, :] = jnp.broadcast_to(rate, (PACK, DK))


def normed_of(mixed, gain):
    mixed = mixed.astype(jnp.bfloat16).astype(jnp.float32)
    mean = jnp.mean(mixed * mixed, axis=-1, keepdims=True)
    return (mixed * lax.rsqrt(mean + norm_eps) * gain).astype(jnp.bfloat16)


def write_halves(place, result_s, near_ref, far_ref):
    tok_count = near_ref.shape[0]
    half = place & 1
    for which, out_ref in ((half, near_ref), (1 - half, far_ref)):
        at = pl.ds(pl.multiple_of(which * tok_count, tok_count), tok_count)
        out_ref[...] = result_s[at, :]


def far_kernel(
    place_ref, gain_ref, got_ref, p2, p3, mixed_b, query_fwd_b, query_bwd_b, fwd_b, bwd_b, end_b, rate_b,
    near_ref, far_ref, value_s, key_s, result_s,
):
    place = place_ref[0]
    size = mixed_b.shape[0]
    arrange(place, value_s, p2, p3, slice(DK, DK + DV))
    arrange(place, key_s, got_ref.at[:size // 2], got_ref.at[size // 2 :], slice(0, DK))
    keys = key_s[...].astype(jnp.float32)
    rates = [rate_b[at : at + 1, :] for at in range(0, rate_b.shape[0], PACK)]
    scores = scores_of(
        in_blocks(query_fwd_b[...]),
        in_blocks(query_bwd_b[...]),
        in_blocks(keys * fwd_b[...]),
        in_blocks(keys * bwd_b[...]),
        in_blocks(keys * end_b[...]),
        rates,
    )
    mixed = mixed_b[...] + dot_nn(scores, value_s[...])
    gain = gain_ref[:, pl.ds(pl.multiple_of(place * DV, DV), DV)]
    result_s[...] = normed_of(mixed, gain)
    write_halves(place, result_s, near_ref, far_ref)


def near_kernel(
    place_ref, gain_ref, got_ref, p2, p3, mixed_a, query_edge_a, edge_b,
    near_ref, far_ref, value_s, key_s, result_s,
):
    place = place_ref[0]
    size = mixed_a.shape[0]
    arrange(place, value_s, p2, p3, slice(DK, DK + DV))
    arrange(place, key_s, got_ref.at[:size // 2], got_ref.at[size // 2 :], slice(0, DK))
    key_edge = (key_s[...].astype(jnp.float32) * edge_b[...]).astype(jnp.bfloat16)
    state = dot_tn(key_edge, value_s[...]).astype(jnp.bfloat16)
    mixed = mixed_a[...] + dot_nn(query_edge_a[...], state)
    gain = gain_ref[:, pl.ds(pl.multiple_of(place * DV, DV), DV)]
    result_s[...] = normed_of(mixed, gain)
    write_halves(place, result_s, near_ref, far_ref)


def on_chip(kernel, place, operands, shapes, scratch):
    return pl.pallas_call(
        kernel,
        in_specs=[pl.BlockSpec(memory_space=pltpu.SMEM)]
        + [pl.BlockSpec(memory_space=pltpu.VMEM)] * len(operands),
        out_specs=[pl.BlockSpec(memory_space=pltpu.VMEM)] * len(shapes),
        out_shape=[jax.ShapeDtypeStruct(*shape) for shape in shapes],
        scratch_shapes=[pltpu.VMEM(*shape) for shape in scratch],
        compiler_params=room(16),
    )(place, *operands)


def mix_heads(place, decay_up, decay_bias, norm_gain, own, got, parcels):
    tok_count = parcels[0].shape[0] - PACK
    size = 2 * tok_count
    rank = decay_up.shape[0]
    short, wide = jnp.bfloat16, jnp.float32
    query, value, mixed = ((size, DK), short), ((size, DV), short), ((size, DV), wide)
    factor = ((size, DK), wide)
    rates = ((size // BLOCK * PACK, DK), wide)
    half = ((tok_count, DV), short)
    (
        mixed_a, mixed_b, query_edge_a, query_fwd_b, query_bwd_b, fwd_b, bwd_b, end_b, edge_b, rate_b,
    ) = on_chip(
        early_kernel,
        place,
        (decay_up, decay_bias.reshape(1, -1), own, *parcels),
        [mixed, mixed, query, query, query, factor, factor, factor, factor, rates],
        [query, value, query, ((4 * rank, size), short), query, ((4 * rank, size), short)],
    )
    gain = norm_gain.reshape(1, -1)
    scratch = [value, query, value]
    far = on_chip(
        far_kernel,
        place,
        (gain, got, *parcels[2:], mixed_b, query_fwd_b, query_bwd_b, fwd_b, bwd_b, end_b, rate_b),
        [half, half],
        scratch,
    )
    near = on_chip(
        near_kernel,
        place,
        (gain, got, *parcels[2:], mixed_a, query_edge_a, edge_b),
        [half, half],
        scratch,
    )
    return [*near, *far]


def join_kernel(place_ref, *refs):
    out_ref = refs[-1]
    for flip, part in enumerate(refs[:-1]):
        at = pl.multiple_of((place_ref[0] ^ flip) * DV, DV)
        out_ref[:, pl.ds(at, DV)] = part[...]


def join_heads(place, parts):
    return pl.pallas_call(
        join_kernel,
        in_specs=[pl.BlockSpec(memory_space=pltpu.SMEM)]
        + [pl.BlockSpec(memory_space=pltpu.VMEM)] * len(parts),
        out_shape=jax.ShapeDtypeStruct((parts[0].shape[0], VAL), jnp.bfloat16),
        compiler_params=room(8),
        name="join",
    )(place, *parts)


def paired_body(
    hidden, queries, values, key_weight, decay_down, decay_up, decay_bias, span_shift, norm_gain
):
    seq_count, tok_count, model_width = hidden.shape
    dp_size = lax.axis_size("dp")
    place = lax.axis_index("sp").reshape(1)
    rank = lax.axis_index("dp").reshape(1)
    token_rows = hidden.reshape(tok_count, model_width)

    peer_rows = exchange(token_rows, "sp", 1)
    own_piece = take_columns(place, key_weight)
    pieces = {0: own_piece}
    for flip in range(2, dp_size, 2):
        pieces[flip] = exchange(own_piece, "dp", flip)
    parcels = make_parcels(
        place,
        token_rows,
        decay_down,
        queries.reshape(tok_count, KEY),
        values.reshape(tok_count, VAL),
        span_shift.reshape(1, tok_count),
    )
    parcels = [parcels[0]] + [exchange(parcels[flip], "sp", flip) for flip in range(1, HEADS)]
    for flip in range(0, dp_size, 2):
        pieces[flip + 1] = exchange(pieces[flip], "dp", 1)
    own, sent = project_keys(rank, token_rows, peer_rows, [pieces[i] for i in range(dp_size)])
    got = exchange(sent, "sp", 2)
    outs = mix_heads(place, decay_up, decay_bias, norm_gain, own, got, parcels)
    parts = [outs[0]] + [exchange(outs[flip], "sp", flip) for flip in range(1, HEADS)]
    return join_heads(place, parts).reshape(seq_count, tok_count, VAL)


def solution(mesh):
    in_specs = (
        P("dp", "sp", None),
        P("dp", "sp", None),
        P("dp", "sp", None),
        P("dp", None),
        P(),
        P(),
        P(),
        P("dp", "sp"),
        P(),
    )
    out_specs = P("dp", "sp", None)
    paired = mesh.shape["sp"] == HEADS and mesh.shape["dp"] % 2 == 0
    body = paired_body if paired else general_body

    return jax.shard_map(body, mesh=mesh, in_specs=in_specs, out_specs=out_specs, check_vma=False)
```

```python
import jax
import jax.numpy as jnp
from jax import lax
from jax.experimental import pallas as pl
from jax.experimental.pallas import tpu as pltpu

from jax.sharding import PartitionSpec as P

HEADS = 4
DK = 256
DV = 512
BLOCK = 64
KEY = 1024
VAL = 2048


decay_tau = 16.0
norm_eps = 1e-05
highest = lax.Precision.HIGHEST


def mechanism(query, keys_in, value_in, log_decay):
    length, key_width = query.shape
    value_width = value_in.shape[-1]
    blocks = length // BLOCK
    step_decay = log_decay.reshape(blocks, BLOCK, key_width)
    inclusive = jnp.cumsum(step_decay, axis=1)
    exclusive = inclusive - step_decay
    total = inclusive[:, -1, :]
    query3 = query.reshape(blocks, BLOCK, key_width)
    keys3 = keys_in.reshape(blocks, BLOCK, key_width)
    value_tensor3 = value_in.reshape(blocks, BLOCK, value_width)
    query_forward_part = (query3 * jnp.exp(inclusive)).astype(jnp.bfloat16)
    key_fwd = (keys3 * jnp.exp(-inclusive)).astype(jnp.bfloat16)
    query_reverse_part = (query3 * jnp.exp(-exclusive)).astype(jnp.bfloat16)
    key_bwd = (keys3 * jnp.exp(exclusive)).astype(jnp.bfloat16)
    key_end = (keys3 * jnp.exp(total[:, None, :] - inclusive)).astype(jnp.bfloat16)
    fwd_scores = jnp.einsum(
        "nid,njd->nij", query_forward_part, key_fwd, preferred_element_type=jnp.float32
    )
    bwd_scores = jnp.einsum(
        "nid,njd->nij", query_reverse_part, key_bwd, preferred_element_type=jnp.float32
    )
    row_index = lax.broadcasted_iota(jnp.int32, (BLOCK, BLOCK), 0)
    col_index = lax.broadcasted_iota(jnp.int32, (BLOCK, BLOCK), 1)
    attention_scores = jnp.where((col_index <= row_index)[None], fwd_scores, bwd_scores).astype(
        jnp.bfloat16
    )
    inner_block_term = jnp.einsum(
        "ucy,uyh->uch", attention_scores, value_tensor3, preferred_element_type=jnp.float32
    )
    end_terms = jnp.einsum(
        "njd,nje->nde", key_end, value_tensor3, preferred_element_type=jnp.float32
    )
    start_terms = jnp.einsum(
        "njd,nje->nde", key_bwd, value_tensor3, preferred_element_type=jnp.float32
    )
    rates = jnp.exp(total)

    def forward_step(carry_state, inputs):
        rate, term = inputs
        return (rate[:, None] * carry_state + term, carry_state)

    def backward_step(carry_state, inputs):
        rate, term = inputs
        state_here = rate[:, None] * carry_state
        return (state_here + term, state_here)

    empty = jnp.zeros((key_width, value_width), jnp.float32)
    _, forward_scan_states = lax.scan(forward_step, empty, (rates, end_terms))
    _, reverse_scan_states = lax.scan(backward_step, empty, (rates, start_terms), reverse=True)
    produced_rows = jnp.einsum(
        "tzv,tvg->tzg",
        query_forward_part,
        forward_scan_states.astype(jnp.bfloat16),
        preferred_element_type=jnp.float32,
    )
    produced_rows = produced_rows + jnp.einsum(
        "tzv,tvg->tzg",
        query_reverse_part,
        reverse_scan_states.astype(jnp.bfloat16),
        preferred_element_type=jnp.float32,
    )
    return (inner_block_term + produced_rows).reshape(length, value_width).astype(jnp.bfloat16)


def general_body(
    hidden, queries, values, key_weight, decay_down, decay_up, decay_bias, span_shift, norm_gain
):
    seq_count, tok_count, model_width = hidden.shape
    group_size = lax.axis_size("sp")
    value_split = group_size // HEADS
    part_width = DV // value_split
    head_index = lax.axis_index("sp") // value_split
    token_rows = hidden.reshape(tok_count, model_width)

    def per_item(tensor, width):
        by_head = tensor.reshape(tok_count, HEADS, width).transpose(1, 0, 2)
        spread_out = jnp.broadcast_to(by_head[:, None], (HEADS, value_split, tok_count, width))
        return spread_out.reshape(group_size, tok_count, width)

    def every_item(tensor):
        return jnp.broadcast_to(tensor[None], (group_size,) + tensor.shape)

    key_sums = jnp.dot(
        token_rows,
        lax.all_gather(key_weight, "dp", axis=0, tiled=True),
        preferred_element_type=jnp.float32,
    )
    keys = key_sums.astype(jnp.bfloat16)
    head_key = lax.all_to_all(per_item(keys, DK), "sp", split_axis=0, concat_axis=1, tiled=True)[0]
    low = jnp.dot(token_rows, decay_down, preferred_element_type=jnp.float32).astype(jnp.bfloat16)
    value_items = values.reshape(tok_count, group_size, part_width).transpose(1, 0, 2)
    head_query, head_value, head_low, head_shift = (
        lax.all_to_all(
            per_item(queries.reshape(tok_count, KEY), DK),
            "sp",
            split_axis=0,
            concat_axis=1,
            tiled=True,
        ),
        lax.all_to_all(value_items, "sp", split_axis=0, concat_axis=1, tiled=True),
        lax.all_to_all(every_item(low), "sp", split_axis=0, concat_axis=1, tiled=True),
        lax.all_to_all(
            every_item(span_shift.reshape(tok_count, 1)),
            "sp",
            split_axis=0,
            concat_axis=1,
            tiled=True,
        ),
    )
    up_columns = lax.dynamic_slice_in_dim(decay_up, head_index * DK, DK, 1)
    bias_part = lax.dynamic_slice_in_dim(decay_bias, head_index * DK, DK, 0)
    pre = jnp.dot(
        head_low[0].astype(jnp.float32),
        up_columns,
        precision=highest,
        preferred_element_type=jnp.float32,
    )
    pre = pre + bias_part[None, :] + head_shift[0].astype(jnp.float32)
    log_decay = jax.nn.log_sigmoid(pre) / decay_tau
    scaled = head_query[0].astype(jnp.float32) * DK ** (-0.5)
    mixed = mechanism(scaled, head_key.astype(jnp.float32), head_value[0], log_decay)
    returned = lax.all_to_all(mixed[None], "sp", split_axis=1, concat_axis=0, tiled=True)
    grouped = returned.astype(jnp.float32).transpose(1, 0, 2).reshape(tok_count, HEADS, DV)
    normed = grouped * lax.rsqrt(jnp.mean(grouped * grouped, axis=-1, keepdims=True) + norm_eps)
    normed = normed * norm_gain.reshape(HEADS, DV)[None]
    return normed.reshape(seq_count, tok_count, VAL).astype(jnp.bfloat16)


PACK = 8


def room(mebibytes):
    return pltpu.CompilerParams(vmem_limit_bytes=mebibytes * 2**20)


def inner(tensors):
    return [pltpu.with_memory_space_constraint(tensor, pltpu.VMEM) for tensor in tensors]


def exchange(tensor, axis, flip):
    size = lax.axis_size(axis)
    return lax.ppermute(tensor, axis, [(i, i ^ flip) for i in range(size)])


def dot_nn(left, right):
    return lax.dot_general(
        left, right, (((1,), (0,)), ((), ())), preferred_element_type=jnp.float32
    )


def dot_nt(left, right):
    return lax.dot_general(
        left, right, (((1,), (1,)), ((), ())), preferred_element_type=jnp.float32
    )


def dot_tn(left, right):
    return lax.dot_general(
        left, right, (((0,), (0,)), ((), ())), preferred_element_type=jnp.float32
    )


def prepare_kernel(
    place_ref, rank_ref, down_ref, shift_ref, up_ref, bias_ref, gain_ref, weight_ref, hidden_ref, query_ref,
    value_ref, piece_ref, hidden_out, up_out, bias_out, gain_out, p0, p1, p2, p3, down_s, shift_s, sems,
):
    parcels = (p0, p1, p2, p3)
    place = place_ref[0]
    tok_count = query_ref.shape[0]
    copies = []

    def fetch(source, target, head=None, width=None):
        if width is not None:
            source = source.at[:, pl.ds(pl.multiple_of(head * width, width), width)]
        copies.append(pltpu.make_async_copy(source, target, sems.at[len(copies)]))
        copies[-1].start()

    fetch(hidden_ref, hidden_out)
    fetch(down_ref, down_s)
    fetch(shift_ref, shift_s)
    for half in range(2):
        fetch(weight_ref, piece_ref.at[:, pl.ds(half * DK, DK)], place ^ (2 * half), DK)
    for flip in (2, 3, 1, 0):
        rows = parcels[flip].at[pl.ds(0, tok_count), :]
        fetch(query_ref, rows.at[:, pl.ds(0, DK)], place ^ flip, DK)
        fetch(value_ref, rows.at[:, pl.ds(DK, DV)], place ^ flip, DV)
    fetch(up_ref, up_out, place, DK)
    fetch(bias_ref, bias_out, place, DK)
    fetch(gain_ref, gain_out, place, DV)
    for copy in copies[:3]:
        copy.wait()
    low = dot_nt(down_s[...], hidden_out[...]).astype(jnp.bfloat16).astype(jnp.float32)
    shift = jnp.broadcast_to(shift_s[...].astype(jnp.float32), (PACK, tok_count))
    empty = jnp.zeros((PACK, DK + DV - 3 * tok_count), jnp.float32)
    tail = jnp.concatenate([low[:PACK], low[PACK:], shift, empty], axis=1).astype(jnp.bfloat16)
    for parcel in parcels:
        parcel[tok_count:, :] = tail
    for copy in copies[3:]:
        copy.wait()


def prepare(place, rank, token_rows, small, key_weight, queries, values):
    tok_count, rows = token_rows.shape[0], key_weight.shape[0]
    down, shift, up, bias, gain = small
    outer = [
        pltpu.with_memory_space_constraint(a, pltpu.HBM)
        for a in (down, shift, up, bias, gain, key_weight, token_rows, queries, values)
    ]
    parcel = jax.ShapeDtypeStruct((tok_count + PACK, DK + DV), jnp.bfloat16)
    shapes = [
        jax.ShapeDtypeStruct((rows, 2 * DK), jnp.bfloat16),
        jax.ShapeDtypeStruct(token_rows.shape, jnp.bfloat16),
        jax.ShapeDtypeStruct((up.shape[0], DK), jnp.float32),
        jax.ShapeDtypeStruct((1, DK), jnp.float32),
        jax.ShapeDtypeStruct((1, DV), jnp.float32),
    ]
    return pl.pallas_call(
        prepare_kernel,
        in_specs=[pl.BlockSpec(memory_space=pltpu.SMEM)] * 2
        + [pl.BlockSpec(memory_space=pl.ANY)] * len(outer),
        out_specs=[pl.BlockSpec(memory_space=pltpu.VMEM)] * (len(shapes) + HEADS),
        out_shape=[pltpu.VMEM(a.shape, a.dtype) for a in shapes + [parcel] * HEADS],
        scratch_shapes=[
            pltpu.VMEM(down.shape, down.dtype),
            pltpu.VMEM(shift.shape, shift.dtype),
            pltpu.SemaphoreType.DMA((8 + 2 * HEADS,)),
        ],
        compiler_params=room(8),
        name="prepare",
    )(place, rank, *outer)


def keys_kernel(rank_ref, hidden_ref, peer_ref, *refs):
    pieces, (own_ref, send_ref) = refs[:-2], refs[-2:]
    tok_count = hidden_ref.shape[0]
    sums = jnp.zeros((2 * tok_count, 2 * DK), jnp.float32)
    for flip, piece in enumerate(pieces):
        rows = piece.shape[0]
        at = pl.multiple_of((rank_ref[0] ^ flip) * rows, rows)
        both = jnp.concatenate([hidden_ref[:, pl.ds(at, rows)], peer_ref[:, pl.ds(at, rows)]], axis=0)
        sums = sums + dot_nn(both, piece[...])
    keys = sums.astype(jnp.bfloat16)
    own_ref[...] = keys[:, :DK]
    send_ref[...] = keys[:, DK:]


def project_keys(rank, token_rows, peer_rows, pieces):
    tok_count = token_rows.shape[0]
    shape = jax.ShapeDtypeStruct((2 * tok_count, DK), jnp.bfloat16)
    return pl.pallas_call(
        keys_kernel,
        in_specs=[pl.BlockSpec(memory_space=pltpu.SMEM)]
        + [pl.BlockSpec(memory_space=pltpu.VMEM)] * (2 + len(pieces)),
        out_shape=[shape, shape],
        compiler_params=room(12),
        name="keys",
    )(rank, *inner((token_rows, peer_rows, *pieces)))


def split3(tensor):
    first = tensor.astype(jnp.bfloat16)
    rest = tensor - first.astype(jnp.float32)
    second = rest.astype(jnp.bfloat16)
    third = (rest - second.astype(jnp.float32)).astype(jnp.bfloat16)
    return first, second, third


def in_blocks(tensor):
    return [tensor[at : at + BLOCK] for at in range(0, tensor.shape[0], BLOCK)]


def arrange(place, target, near, far):
    tok_count = target.shape[0] // 2
    half = place & 1
    for which, part in ((half, near), (1 - half, far)):
        at = pl.ds(pl.multiple_of(which * tok_count, tok_count), tok_count)
        target[at, :] = part[...]


def query_of(parcel):
    return parcel.at[: parcel.shape[0] - PACK, :DK]


def value_of(parcel):
    return parcel.at[: parcel.shape[0] - PACK, DK:]


def arrange_low(place, near, far):
    tok_count = near.shape[0] - PACK
    near, far = (part[tok_count:, :].astype(jnp.float32) for part in (near, far))
    odd = (place & 1) == 1
    halves = []
    for part in (jnp.where(odd, far, near), jnp.where(odd, near, far)):
        low = [part[:, :tok_count], part[:, tok_count : 2 * tok_count]]
        shift = part[:, 2 * tok_count : 3 * tok_count]
        row = lax.broadcasted_iota(jnp.int32, shift.shape, 0)
        first = jnp.where(row == 0, shift, 0.0)
        halves.append(jnp.concatenate(low * 3 + [first, jnp.zeros_like(first)], axis=0))
    return jnp.concatenate(halves, axis=1).astype(jnp.bfloat16)


def decay_of(low, up, bias, sum_up_to):
    pre = dot_tn(low, up) + bias
    decay = (jnp.minimum(pre, 0.0) - jnp.log1p(jnp.exp(-jnp.abs(pre)))) * (1.0 / decay_tau)
    inclusive = sum(dot_nn(sum_up_to, part) for part in split3(decay))
    return decay, inclusive


def scores_of(query_fwd, query_bwd, key_fwd, key_bwd, key_end, rates):
    blocks = len(rates)
    short = lambda tensors: [tensor.astype(jnp.bfloat16) for tensor in tensors]
    key_fwd, near_bwd = short(key_fwd), short(key_bwd)
    width = blocks * BLOCK
    row = lax.broadcasted_iota(jnp.int32, (BLOCK, width), 0)
    col = lax.broadcasted_iota(jnp.int32, (BLOCK, width), 1)
    rows = []
    for here in range(blocks):
        left, right = list(key_fwd), list(near_bwd)
        for past in range(here):
            faded = key_end[past]
            for between in range(past + 1, here):
                faded = faded * rates[between]
            left[past] = faded.astype(jnp.bfloat16)
        fade = None
        for later in range(here + 1, blocks):
            fade = rates[later - 1] if fade is None else fade * rates[later - 1]
            right[later] = (key_bwd[later] * fade).astype(jnp.bfloat16)
        fwd = dot_nt(query_fwd[here], jnp.concatenate(left, axis=0))
        bwd = dot_nt(query_bwd[here], jnp.concatenate(right, axis=0))
        rows.append(jnp.where(col <= row + here * BLOCK, fwd, bwd).astype(jnp.bfloat16))
    return jnp.concatenate(rows, axis=0)


def factors(decay, inclusive, facing_right):
    blocks = zip(in_blocks(decay), in_blocks(inclusive))
    decay, inclusive = map(list, zip(*blocks))
    totals = [tensor[BLOCK - 1 :] for tensor in inclusive]
    none = jnp.zeros_like(totals[0])
    right = jnp.where(facing_right, 1.0, 0.0)
    found = []
    for at in range(len(totals)):
        exclusive = inclusive[at] - decay[at]
        before = sum(totals[:at], none)
        after = sum(totals[at:], none)
        base = right * after + (1.0 - right) * before
        sign = 1.0 - 2.0 * right
        found.append(
            dict(
                query_fwd=jnp.exp(inclusive[at]),
                query_bwd=jnp.exp(-exclusive),
                key_fwd=jnp.exp(-inclusive[at]),
                key_bwd=jnp.exp(exclusive),
                key_end=jnp.exp(totals[at] - inclusive[at]),
                key_edge=jnp.exp(base + sign * (exclusive + right * decay[at])),
                query_edge=jnp.exp(base + sign * (inclusive[at] - right * decay[at])),
                rate=jnp.exp(totals[at]),
            )
        )
    return {name: [one[name] for one in found] for name in found[0]}


def decay_inputs(up_ref, bias_ref, size):
    rank = up_ref.shape[0]
    ones = (lax.broadcasted_iota(jnp.int32, (rank, DK), 0) == 0).astype(jnp.float32)
    up = jnp.concatenate(
        [part.astype(jnp.float32) for part in split3(up_ref[...])] + [ones], axis=0
    ).astype(jnp.bfloat16)
    row = lax.broadcasted_iota(jnp.int32, (size, size), 0)
    col = lax.broadcasted_iota(jnp.int32, (size, size), 1)
    lower = ((row // BLOCK) == (col // BLOCK)) & (col <= row)
    return up, bias_ref[...], jnp.where(lower, 1.0, 0.0).astype(jnp.bfloat16)


def joined(tensors):
    return jnp.concatenate(tensors, axis=0)


def times(left, right):
    return [a * b for a, b in zip(left, right)]


def short(tensors):
    return [tensor.astype(jnp.bfloat16) for tensor in tensors]


def own_kernel(
    place_ref, up_ref, bias_ref, own_ref, p0, p1,
    mixed_a, query_edge_a, state_a, query_s, value_s, key_s,
):
    place = place_ref[0]
    size = mixed_a.shape[0]
    arrange(place, query_s, query_of(p0), query_of(p1))
    arrange(place, value_s, value_of(p0), value_of(p1))
    arrange(place, key_s, own_ref.at[: size // 2], own_ref.at[size // 2 :])
    up, bias, sum_up_to = decay_inputs(up_ref, bias_ref, size)
    low = arrange_low(place, p0, p1)
    found = factors(*decay_of(low, up, bias, sum_up_to), place < HEADS // 2)
    scaled = in_blocks(query_s[...].astype(jnp.float32) * DK**-0.5)
    keys = in_blocks(key_s[...].astype(jnp.float32))
    scores = scores_of(
        short(times(scaled, found["query_fwd"])),
        short(times(scaled, found["query_bwd"])),
        times(keys, found["key_fwd"]),
        times(keys, found["key_bwd"]),
        times(keys, found["key_end"]),
        found["rate"],
    )
    mixed_a[...] = dot_nn(scores, value_s[...])
    query_edge_a[...] = joined(short(times(scaled, found["query_edge"])))
    key_edge = joined(short(times(keys, found["key_edge"])))
    state_a[...] = dot_tn(key_edge, value_s[...]).astype(jnp.bfloat16)


def other_kernel(
    place_ref, up_ref, bias_ref, state_a, p2, p3,
    mixed_b, query_fwd_b, query_bwd_b, fwd_b, bwd_b, end_b, edge_b, rate_b, query_s,
):
    place = place_ref[0]
    arrange(place, query_s, query_of(p2), query_of(p3))
    up, bias, sum_up_to = decay_inputs(up_ref, bias_ref, mixed_b.shape[0])
    low = arrange_low(place, p2, p3)
    found = factors(*decay_of(low, up, bias, sum_up_to), place >= HEADS // 2)
    scaled = in_blocks(query_s[...].astype(jnp.float32) * DK**-0.5)
    query_fwd_b[...] = joined(short(times(scaled, found["query_fwd"])))
    query_bwd_b[...] = joined(short(times(scaled, found["query_bwd"])))
    mixed_b[...] = dot_nn(joined(short(times(scaled, found["query_edge"]))), state_a[...])
    fwd_b[...] = joined(found["key_fwd"])
    bwd_b[...] = joined(found["key_bwd"])
    end_b[...] = joined(found["key_end"])
    edge_b[...] = joined(found["key_edge"])
    for at, rate in enumerate(found["rate"]):
        rate_b[at * PACK : (at + 1) * PACK, :] = jnp.broadcast_to(rate, (PACK, DK))


def normed_of(mixed, gain):
    mixed = mixed.astype(jnp.bfloat16).astype(jnp.float32)
    mean = jnp.mean(mixed * mixed, axis=-1, keepdims=True)
    return (mixed * lax.rsqrt(mean + norm_eps) * gain).astype(jnp.bfloat16)


def write_halves(place, result_s, near_ref, far_ref):
    tok_count = near_ref.shape[0]
    half = place & 1
    for which, out_ref in ((half, near_ref), (1 - half, far_ref)):
        at = pl.ds(pl.multiple_of(which * tok_count, tok_count), tok_count)
        out_ref[...] = result_s[at, :]


def far_kernel(
    place_ref, gain_ref, got_ref, p2, p3, mixed_b, query_fwd_b, query_bwd_b, fwd_b, bwd_b, end_b, rate_b,
    near_ref, far_ref, value_s, key_s, result_s,
):
    place = place_ref[0]
    size = mixed_b.shape[0]
    arrange(place, value_s, value_of(p2), value_of(p3))
    arrange(place, key_s, got_ref.at[: size // 2], got_ref.at[size // 2 :])
    keys = key_s[...].astype(jnp.float32)
    rates = [rate_b[at : at + 1, :] for at in range(0, rate_b.shape[0], PACK)]
    scores = scores_of(
        in_blocks(query_fwd_b[...]),
        in_blocks(query_bwd_b[...]),
        in_blocks(keys * fwd_b[...]),
        in_blocks(keys * bwd_b[...]),
        in_blocks(keys * end_b[...]),
        rates,
    )
    mixed = mixed_b[...] + dot_nn(scores, value_s[...])
    result_s[...] = normed_of(mixed, gain_ref[...])
    write_halves(place, result_s, near_ref, far_ref)


def near_kernel(
    place_ref, gain_ref, got_ref, p2, p3, mixed_a, query_edge_a, edge_b,
    near_ref, far_ref, value_s, key_s, result_s,
):
    place = place_ref[0]
    size = mixed_a.shape[0]
    arrange(place, value_s, value_of(p2), value_of(p3))
    arrange(place, key_s, got_ref.at[: size // 2], got_ref.at[size // 2 :])
    key_edge = (key_s[...].astype(jnp.float32) * edge_b[...]).astype(jnp.bfloat16)
    state = dot_tn(key_edge, value_s[...]).astype(jnp.bfloat16)
    mixed = mixed_a[...] + dot_nn(query_edge_a[...], state)
    result_s[...] = normed_of(mixed, gain_ref[...])
    write_halves(place, result_s, near_ref, far_ref)


def on_chip(kernel, place, operands, shapes, scratch):
    return pl.pallas_call(
        kernel,
        in_specs=[pl.BlockSpec(memory_space=pltpu.SMEM)]
        + [pl.BlockSpec(memory_space=pltpu.VMEM)] * len(operands),
        out_specs=[pl.BlockSpec(memory_space=pltpu.VMEM)] * len(shapes),
        out_shape=[jax.ShapeDtypeStruct(*shape) for shape in shapes],
        scratch_shapes=[pltpu.VMEM(*shape) for shape in scratch],
        compiler_params=room(16),
    )(place, *inner(operands))


def mix_heads(place, up, bias, gain, own, got, parcels):
    tok_count = parcels[0].shape[0] - PACK
    size = 2 * tok_count
    narrow, wide = jnp.bfloat16, jnp.float32
    query, value, mixed = ((size, DK), narrow), ((size, DV), narrow), ((size, DV), wide)
    factor, state = ((size, DK), wide), ((DK, DV), narrow)
    rates = ((size // BLOCK * PACK, DK), wide)
    half = ((tok_count, DV), narrow)
    mixed_a, query_edge_a, state_a = on_chip(
        own_kernel,
        place,
        (up, bias, own, *parcels[:2]),
        [mixed, query, state],
        [query, value, query],
    )
    mixed_b, query_fwd_b, query_bwd_b, fwd_b, bwd_b, end_b, edge_b, rate_b = on_chip(
        other_kernel,
        place,
        (up, bias, state_a, *parcels[2:]),
        [mixed, query, query, factor, factor, factor, factor, rates],
        [query],
    )
    scratch = [value, query, value]
    far = on_chip(
        far_kernel,
        place,
        (gain, got, *parcels[2:], mixed_b, query_fwd_b, query_bwd_b, fwd_b, bwd_b, end_b, rate_b),
        [half, half],
        scratch,
    )
    near = on_chip(
        near_kernel,
        place,
        (gain, got, *parcels[2:], mixed_a, query_edge_a, edge_b),
        [half, half],
        scratch,
    )
    return [*near, *far]


def join_kernel(place_ref, *refs):
    out_ref = refs[-1]
    for flip, part in enumerate(refs[:-1]):
        at = pl.multiple_of((place_ref[0] ^ flip) * DV, DV)
        out_ref[:, pl.ds(at, DV)] = part[...]


def join_heads(place, parts):
    return pl.pallas_call(
        join_kernel,
        in_specs=[pl.BlockSpec(memory_space=pltpu.SMEM)]
        + [pl.BlockSpec(memory_space=pltpu.VMEM)] * len(parts),
        out_shape=jax.ShapeDtypeStruct((parts[0].shape[0], VAL), jnp.bfloat16),
        compiler_params=room(8),
        name="join",
    )(place, *parts)


def paired_body(
    hidden, queries, values, key_weight, decay_down, decay_up, decay_bias, span_shift, norm_gain
):
    seq_count, tok_count, model_width = hidden.shape
    dp_size = lax.axis_size("dp")
    place = lax.axis_index("sp").reshape(1)
    rank = lax.axis_index("dp").reshape(1)
    token_rows = hidden.reshape(tok_count, model_width)

    small = (
        decay_down.T,
        span_shift.reshape(1, tok_count),
        decay_up,
        decay_bias.reshape(1, -1),
        norm_gain.reshape(1, -1),
    )
    own_piece, own_rows, up, bias, gain, *parcels = prepare(
        place,
        rank,
        token_rows,
        small,
        key_weight,
        queries.reshape(tok_count, KEY),
        values.reshape(tok_count, VAL),
    )
    peer_rows = exchange(token_rows, "sp", 1)
    pieces = {0: own_piece}
    for flip in range(2, dp_size, 2):
        pieces[flip] = exchange(own_piece, "dp", flip)
    parcels = [parcels[0]] + [exchange(parcels[flip], "sp", flip) for flip in range(1, HEADS)]
    for flip in range(0, dp_size, 2):
        pieces[flip + 1] = exchange(pieces[flip], "dp", 1)
    own, sent = project_keys(rank, own_rows, peer_rows, [pieces[i] for i in range(dp_size)])
    got = exchange(sent, "sp", 2)
    outs = mix_heads(place, up, bias, gain, own, got, parcels)
    parts = [outs[0]] + [exchange(outs[flip], "sp", flip) for flip in range(1, HEADS)]
    return join_heads(place, parts).reshape(seq_count, tok_count, VAL)


def solution(mesh):
    in_specs = (
        P("dp", "sp", None),
        P("dp", "sp", None),
        P("dp", "sp", None),
        P("dp", None),
        P(),
        P(),
        P(),
        P("dp", "sp"),
        P(),
    )
    out_specs = P("dp", "sp", None)
    paired = mesh.shape["sp"] == HEADS and mesh.shape["dp"] % 2 == 0
    body = paired_body if paired else general_body

    return jax.shard_map(body, mesh=mesh, in_specs=in_specs, out_specs=out_specs, check_vma=False)
```

```python
import jax
import jax.numpy as jnp
from jax import lax
from jax.experimental import pallas as pl
from jax.experimental.pallas import tpu as pltpu

from jax.sharding import PartitionSpec as P

HEADS = 4
DK = 256
DV = 512
BLOCK = 64
KEY = 1024
VAL = 2048


decay_tau = 16.0
norm_eps = 1e-05
highest = lax.Precision.HIGHEST


def mechanism(query, keys_in, value_in, log_decay):
    length, key_width = query.shape
    value_width = value_in.shape[-1]
    blocks = length // BLOCK
    step_decay = log_decay.reshape(blocks, BLOCK, key_width)
    inclusive = jnp.cumsum(step_decay, axis=1)
    exclusive = inclusive - step_decay
    total = inclusive[:, -1, :]
    query3 = query.reshape(blocks, BLOCK, key_width)
    keys3 = keys_in.reshape(blocks, BLOCK, key_width)
    value_tensor3 = value_in.reshape(blocks, BLOCK, value_width)
    query_forward_part = (query3 * jnp.exp(inclusive)).astype(jnp.bfloat16)
    key_fwd = (keys3 * jnp.exp(-inclusive)).astype(jnp.bfloat16)
    query_reverse_part = (query3 * jnp.exp(-exclusive)).astype(jnp.bfloat16)
    key_bwd = (keys3 * jnp.exp(exclusive)).astype(jnp.bfloat16)
    key_end = (keys3 * jnp.exp(total[:, None, :] - inclusive)).astype(jnp.bfloat16)
    fwd_scores = jnp.einsum(
        "nid,njd->nij", query_forward_part, key_fwd, preferred_element_type=jnp.float32
    )
    bwd_scores = jnp.einsum(
        "nid,njd->nij", query_reverse_part, key_bwd, preferred_element_type=jnp.float32
    )
    row_index = lax.broadcasted_iota(jnp.int32, (BLOCK, BLOCK), 0)
    col_index = lax.broadcasted_iota(jnp.int32, (BLOCK, BLOCK), 1)
    attention_scores = jnp.where((col_index <= row_index)[None], fwd_scores, bwd_scores).astype(
        jnp.bfloat16
    )
    inner_block_term = jnp.einsum(
        "ucy,uyh->uch", attention_scores, value_tensor3, preferred_element_type=jnp.float32
    )
    end_terms = jnp.einsum(
        "njd,nje->nde", key_end, value_tensor3, preferred_element_type=jnp.float32
    )
    start_terms = jnp.einsum(
        "njd,nje->nde", key_bwd, value_tensor3, preferred_element_type=jnp.float32
    )
    rates = jnp.exp(total)

    def forward_step(carry_state, inputs):
        rate, term = inputs
        return (rate[:, None] * carry_state + term, carry_state)

    def backward_step(carry_state, inputs):
        rate, term = inputs
        state_here = rate[:, None] * carry_state
        return (state_here + term, state_here)

    empty = jnp.zeros((key_width, value_width), jnp.float32)
    _, forward_scan_states = lax.scan(forward_step, empty, (rates, end_terms))
    _, reverse_scan_states = lax.scan(backward_step, empty, (rates, start_terms), reverse=True)
    produced_rows = jnp.einsum(
        "tzv,tvg->tzg",
        query_forward_part,
        forward_scan_states.astype(jnp.bfloat16),
        preferred_element_type=jnp.float32,
    )
    produced_rows = produced_rows + jnp.einsum(
        "tzv,tvg->tzg",
        query_reverse_part,
        reverse_scan_states.astype(jnp.bfloat16),
        preferred_element_type=jnp.float32,
    )
    return (inner_block_term + produced_rows).reshape(length, value_width).astype(jnp.bfloat16)


def general_body(
    hidden, queries, values, key_weight, decay_down, decay_up, decay_bias, span_shift, norm_gain
):
    seq_count, tok_count, model_width = hidden.shape
    group_size = lax.axis_size("sp")
    value_split = group_size // HEADS
    part_width = DV // value_split
    head_index = lax.axis_index("sp") // value_split
    token_rows = hidden.reshape(tok_count, model_width)

    def per_item(tensor, width):
        by_head = tensor.reshape(tok_count, HEADS, width).transpose(1, 0, 2)
        spread_out = jnp.broadcast_to(by_head[:, None], (HEADS, value_split, tok_count, width))
        return spread_out.reshape(group_size, tok_count, width)

    def every_item(tensor):
        return jnp.broadcast_to(tensor[None], (group_size,) + tensor.shape)

    key_sums = jnp.dot(
        token_rows,
        lax.all_gather(key_weight, "dp", axis=0, tiled=True),
        preferred_element_type=jnp.float32,
    )
    keys = key_sums.astype(jnp.bfloat16)
    head_key = lax.all_to_all(per_item(keys, DK), "sp", split_axis=0, concat_axis=1, tiled=True)[0]
    low = jnp.dot(token_rows, decay_down, preferred_element_type=jnp.float32).astype(jnp.bfloat16)
    value_items = values.reshape(tok_count, group_size, part_width).transpose(1, 0, 2)
    head_query, head_value, head_low, head_shift = (
        lax.all_to_all(
            per_item(queries.reshape(tok_count, KEY), DK),
            "sp",
            split_axis=0,
            concat_axis=1,
            tiled=True,
        ),
        lax.all_to_all(value_items, "sp", split_axis=0, concat_axis=1, tiled=True),
        lax.all_to_all(every_item(low), "sp", split_axis=0, concat_axis=1, tiled=True),
        lax.all_to_all(
            every_item(span_shift.reshape(tok_count, 1)),
            "sp",
            split_axis=0,
            concat_axis=1,
            tiled=True,
        ),
    )
    up_columns = lax.dynamic_slice_in_dim(decay_up, head_index * DK, DK, 1)
    bias_part = lax.dynamic_slice_in_dim(decay_bias, head_index * DK, DK, 0)
    pre = jnp.dot(
        head_low[0].astype(jnp.float32),
        up_columns,
        precision=highest,
        preferred_element_type=jnp.float32,
    )
    pre = pre + bias_part[None, :] + head_shift[0].astype(jnp.float32)
    log_decay = jax.nn.log_sigmoid(pre) / decay_tau
    scaled = head_query[0].astype(jnp.float32) * DK ** (-0.5)
    mixed = mechanism(scaled, head_key.astype(jnp.float32), head_value[0], log_decay)
    returned = lax.all_to_all(mixed[None], "sp", split_axis=1, concat_axis=0, tiled=True)
    grouped = returned.astype(jnp.float32).transpose(1, 0, 2).reshape(tok_count, HEADS, DV)
    normed = grouped * lax.rsqrt(jnp.mean(grouped * grouped, axis=-1, keepdims=True) + norm_eps)
    normed = normed * norm_gain.reshape(HEADS, DV)[None]
    return normed.reshape(seq_count, tok_count, VAL).astype(jnp.bfloat16)


PACK = 8


def room(mebibytes):
    return pltpu.CompilerParams(vmem_limit_bytes=mebibytes * 2**20)


def inner(tensors):
    return [pltpu.with_memory_space_constraint(tensor, pltpu.VMEM) for tensor in tensors]


def exchange(tensor, axis, flip):
    size = lax.axis_size(axis)
    return lax.ppermute(tensor, axis, [(i, i ^ flip) for i in range(size)])


def dot_nn(left, right):
    return lax.dot_general(
        left, right, (((1,), (0,)), ((), ())), preferred_element_type=jnp.float32
    )


def dot_nt(left, right):
    return lax.dot_general(
        left, right, (((1,), (1,)), ((), ())), preferred_element_type=jnp.float32
    )


def dot_tn(left, right):
    return lax.dot_general(
        left, right, (((0,), (0,)), ((), ())), preferred_element_type=jnp.float32
    )


def prepare_kernel(
    place_ref, rank_ref, down_ref, shift_ref, up_ref, bias_ref, gain_ref, weight_ref, hidden_ref, query_ref,
    value_ref, own_piece, sent_piece, hidden_out, up_out, bias_out, gain_out, p0, p1, p2, p3, down_s, shift_s, sems,
):
    parcels = (p0, p1, p2, p3)
    place = place_ref[0]
    tok_count = query_ref.shape[0]
    copies = []

    def fetch(source, target, head=None, width=None):
        if width is not None:
            source = source.at[:, pl.ds(pl.multiple_of(head * width, width), width)]
        copies.append(pltpu.make_async_copy(source, target, sems.at[len(copies)]))
        copies[-1].start()

    fetch(hidden_ref, hidden_out)
    fetch(down_ref, down_s)
    fetch(shift_ref, shift_s)
    fetch(weight_ref, sent_piece, place ^ 2, DK)
    fetch(weight_ref, own_piece, place, DK)
    for flip in (2, 3, 1, 0):
        head = place ^ flip
        sources = ((query_ref, head), (value_ref, 2 * head), (value_ref, 2 * head + 1))
        for slot, (source, column) in enumerate(sources):
            rows = parcels[flip].at[pl.ds(slot * tok_count, tok_count), :]
            fetch(source, rows, column, DK)
    fetch(up_ref, up_out, place, DK)
    fetch(bias_ref, bias_out, place, DK)
    fetch(gain_ref, gain_out, place, DV)
    for copy in copies[:3]:
        copy.wait()
    low = dot_nt(down_s[...], hidden_out[...]).astype(jnp.bfloat16).astype(jnp.float32)
    shift = jnp.broadcast_to(shift_s[...].astype(jnp.float32), (PACK, tok_count))
    low = jnp.concatenate([low[:PACK], low[PACK:]], axis=1)
    shift = jnp.concatenate([shift, shift], axis=1)
    tail = jnp.concatenate([low, shift], axis=0).astype(jnp.bfloat16)
    for parcel in parcels:
        parcel[3 * tok_count :, :] = tail
    for copy in copies[3:]:
        copy.wait()


def prepare(place, rank, token_rows, small, key_weight, queries, values):
    tok_count, rows = token_rows.shape[0], key_weight.shape[0]
    down, shift, up, bias, gain = small
    outer = [
        pltpu.with_memory_space_constraint(a, pltpu.HBM)
        for a in (down, shift, up, bias, gain, key_weight, token_rows, queries, values)
    ]
    parcel = jax.ShapeDtypeStruct((3 * tok_count + 2 * PACK, DK), jnp.bfloat16)
    shapes = [
        jax.ShapeDtypeStruct((rows, DK), jnp.bfloat16),
        jax.ShapeDtypeStruct((rows, DK), jnp.bfloat16),
        jax.ShapeDtypeStruct(token_rows.shape, jnp.bfloat16),
        jax.ShapeDtypeStruct((up.shape[0], DK), jnp.float32),
        jax.ShapeDtypeStruct((1, DK), jnp.float32),
        jax.ShapeDtypeStruct((1, DV), jnp.float32),
    ]
    return pl.pallas_call(
        prepare_kernel,
        in_specs=[pl.BlockSpec(memory_space=pltpu.SMEM)] * 2
        + [pl.BlockSpec(memory_space=pl.ANY)] * len(outer),
        out_specs=[pl.BlockSpec(memory_space=pltpu.VMEM)] * (len(shapes) + HEADS),
        out_shape=[pltpu.VMEM(a.shape, a.dtype) for a in shapes + [parcel] * HEADS],
        scratch_shapes=[
            pltpu.VMEM(down.shape, down.dtype),
            pltpu.VMEM(shift.shape, shift.dtype),
            pltpu.SemaphoreType.DMA((8 + 3 * HEADS,)),
        ],
        compiler_params=room(8),
        name="prepare",
    )(place, rank, *outer)


def keys_kernel(rank_ref, *refs):
    count = lax.axis_size("dp")
    sets = (len(refs) - count) // 2
    pieces = refs[sets : sets + count]
    for tokens, keys in zip(refs[:sets], refs[sets + count :]):
        sums = jnp.zeros(keys.shape, jnp.float32)
        for flip, piece in enumerate(pieces):
            rows = piece.shape[0]
            at = pl.multiple_of((rank_ref[0] ^ flip) * rows, rows)
            sums = sums + dot_nn(tokens[:, pl.ds(at, rows)], piece[...])
        keys[...] = sums.astype(jnp.bfloat16)


def project_keys(rank, tokens, pieces):
    operands = (*tokens, *pieces)
    return pl.pallas_call(
        keys_kernel,
        in_specs=[pl.BlockSpec(memory_space=pltpu.SMEM)]
        + [pl.BlockSpec(memory_space=pltpu.VMEM)] * len(operands),
        out_shape=[jax.ShapeDtypeStruct((rows.shape[0], DK), jnp.bfloat16) for rows in tokens],
        compiler_params=room(12),
        name="keys",
    )(rank, *inner(operands))


def split3(tensor):
    first = tensor.astype(jnp.bfloat16)
    rest = tensor - first.astype(jnp.float32)
    second = rest.astype(jnp.bfloat16)
    third = (rest - second.astype(jnp.float32)).astype(jnp.bfloat16)
    return first, second, third


def in_blocks(tensor):
    return [tensor[at : at + BLOCK] for at in range(0, tensor.shape[0], BLOCK)]


def arrange(place, target, near, far):
    tok_count = target.shape[0] // 2
    half = place & 1
    for which, part in ((half, near), (1 - half, far)):
        at = pl.ds(pl.multiple_of(which * tok_count, tok_count), tok_count)
        target[at, :] = part[...]


def tokens_of(parcel):
    return (parcel.shape[0] - 2 * PACK) // 3


def query_of(parcel):
    return parcel.at[: tokens_of(parcel), :]


def arrange_values(place, target, near, far):
    tok_count = target.shape[0] // 2
    half = place & 1
    for which, part in ((half, near), (1 - half, far)):
        at = pl.ds(pl.multiple_of(which * tok_count, tok_count), tok_count)
        target[at, :DK] = part[tok_count : 2 * tok_count, :]
        target[at, DK:] = part[2 * tok_count : 3 * tok_count, :]


def arrange_low(place, near, far):
    tok_count = tokens_of(near)
    near, far = (part[3 * tok_count :, :].astype(jnp.float32) for part in (near, far))
    odd = (place & 1) == 1
    halves = []
    for part in (jnp.where(odd, far, near), jnp.where(odd, near, far)):
        low = [part[:PACK, :tok_count], part[:PACK, tok_count:]]
        shift = part[PACK:, :tok_count]
        row = lax.broadcasted_iota(jnp.int32, shift.shape, 0)
        first = jnp.where(row == 0, shift, 0.0)
        halves.append(jnp.concatenate(low * 3 + [first, jnp.zeros_like(first)], axis=0))
    return jnp.concatenate(halves, axis=1).astype(jnp.bfloat16)


def decay_of(low, up, bias, sum_up_to):
    pre = dot_tn(low, up) + bias
    decay = (jnp.minimum(pre, 0.0) - jnp.log1p(jnp.exp(-jnp.abs(pre)))) * (1.0 / decay_tau)
    inclusive = sum(dot_nn(sum_up_to, part) for part in split3(decay))
    return decay, inclusive


def scores_of(query_fwd, query_bwd, key_fwd, key_bwd, key_end, rates):
    blocks = len(rates)
    short = lambda tensors: [tensor.astype(jnp.bfloat16) for tensor in tensors]
    key_fwd, near_bwd = short(key_fwd), short(key_bwd)
    width = blocks * BLOCK
    row = lax.broadcasted_iota(jnp.int32, (BLOCK, width), 0)
    col = lax.broadcasted_iota(jnp.int32, (BLOCK, width), 1)
    rows = []
    for here in range(blocks):
        left, right = list(key_fwd), list(near_bwd)
        for past in range(here):
            faded = key_end[past]
            for between in range(past + 1, here):
                faded = faded * rates[between]
            left[past] = faded.astype(jnp.bfloat16)
        fade = None
        for later in range(here + 1, blocks):
            fade = rates[later - 1] if fade is None else fade * rates[later - 1]
            right[later] = (key_bwd[later] * fade).astype(jnp.bfloat16)
        fwd = dot_nt(query_fwd[here], jnp.concatenate(left, axis=0))
        bwd = dot_nt(query_bwd[here], jnp.concatenate(right, axis=0))
        rows.append(jnp.where(col <= row + here * BLOCK, fwd, bwd).astype(jnp.bfloat16))
    return jnp.concatenate(rows, axis=0)


def factors(decay, inclusive, facing_right):
    blocks = zip(in_blocks(decay), in_blocks(inclusive))
    decay, inclusive = map(list, zip(*blocks))
    totals = [tensor[BLOCK - 1 :] for tensor in inclusive]
    none = jnp.zeros_like(totals[0])
    right = jnp.where(facing_right, 1.0, 0.0)
    found = []
    for at in range(len(totals)):
        exclusive = inclusive[at] - decay[at]
        before = sum(totals[:at], none)
        after = sum(totals[at:], none)
        base = right * after + (1.0 - right) * before
        sign = 1.0 - 2.0 * right
        found.append(
            dict(
                query_fwd=jnp.exp(inclusive[at]),
                query_bwd=jnp.exp(-exclusive),
                key_fwd=jnp.exp(-inclusive[at]),
                key_bwd=jnp.exp(exclusive),
                key_end=jnp.exp(totals[at] - inclusive[at]),
                key_edge=jnp.exp(base + sign * (exclusive + right * decay[at])),
                query_edge=jnp.exp(base + sign * (inclusive[at] - right * decay[at])),
                rate=jnp.exp(totals[at]),
            )
        )
    return {name: [one[name] for one in found] for name in found[0]}


def decay_inputs(up_ref, bias_ref, size):
    rank = up_ref.shape[0]
    ones = (lax.broadcasted_iota(jnp.int32, (rank, DK), 0) == 0).astype(jnp.float32)
    up = jnp.concatenate(
        [part.astype(jnp.float32) for part in split3(up_ref[...])] + [ones], axis=0
    ).astype(jnp.bfloat16)
    row = lax.broadcasted_iota(jnp.int32, (size, size), 0)
    col = lax.broadcasted_iota(jnp.int32, (size, size), 1)
    lower = ((row // BLOCK) == (col // BLOCK)) & (col <= row)
    return up, bias_ref[...], jnp.where(lower, 1.0, 0.0).astype(jnp.bfloat16)


def joined(tensors):
    return jnp.concatenate(tensors, axis=0)


def times(left, right):
    return [a * b for a, b in zip(left, right)]


def short(tensors):
    return [tensor.astype(jnp.bfloat16) for tensor in tensors]


def own_kernel(
    place_ref, up_ref, bias_ref, near_keys, far_keys, p0, p1,
    mixed_a, query_edge_a, state_a, query_s, value_s, key_s,
):
    place = place_ref[0]
    size = mixed_a.shape[0]
    arrange(place, query_s, query_of(p0), query_of(p1))
    arrange_values(place, value_s, p0, p1)
    arrange(place, key_s, near_keys, far_keys)
    up, bias, sum_up_to = decay_inputs(up_ref, bias_ref, size)
    low = arrange_low(place, p0, p1)
    found = factors(*decay_of(low, up, bias, sum_up_to), place < HEADS // 2)
    scaled = in_blocks(query_s[...].astype(jnp.float32) * DK**-0.5)
    keys = in_blocks(key_s[...].astype(jnp.float32))
    scores = scores_of(
        short(times(scaled, found["query_fwd"])),
        short(times(scaled, found["query_bwd"])),
        times(keys, found["key_fwd"]),
        times(keys, found["key_bwd"]),
        times(keys, found["key_end"]),
        found["rate"],
    )
    mixed_a[...] = dot_nn(scores, value_s[...])
    query_edge_a[...] = joined(short(times(scaled, found["query_edge"])))
    key_edge = joined(short(times(keys, found["key_edge"])))
    state_a[...] = dot_tn(key_edge, value_s[...]).astype(jnp.bfloat16)


def other_kernel(
    place_ref, up_ref, bias_ref, state_a, p2, p3,
    mixed_b, query_fwd_b, query_bwd_b, fwd_b, bwd_b, end_b, edge_b, rate_b, query_s,
):
    place = place_ref[0]
    arrange(place, query_s, query_of(p2), query_of(p3))
    up, bias, sum_up_to = decay_inputs(up_ref, bias_ref, query_s.shape[0])
    low = arrange_low(place, p2, p3)
    found = factors(*decay_of(low, up, bias, sum_up_to), place >= HEADS // 2)
    scaled = in_blocks(query_s[...].astype(jnp.float32) * DK**-0.5)
    query_fwd_b[...] = joined(short(times(scaled, found["query_fwd"])))
    query_bwd_b[...] = joined(short(times(scaled, found["query_bwd"])))
    mixed_b[...] = dot_nn(joined(short(times(scaled, found["query_edge"]))), state_a[...])
    fwd_b[...] = joined(found["key_fwd"])
    bwd_b[...] = joined(found["key_bwd"])
    end_b[...] = joined(found["key_end"])
    edge_b[...] = joined(found["key_edge"])
    for at, rate in enumerate(found["rate"]):
        rate_b[at * PACK : (at + 1) * PACK, :] = jnp.broadcast_to(rate, (PACK, DK))


def normed_of(mixed, gain):
    mixed = mixed.astype(jnp.bfloat16).astype(jnp.float32)
    mean = jnp.mean(mixed * mixed, axis=-1, keepdims=True)
    return (mixed * lax.rsqrt(mean + norm_eps) * gain).astype(jnp.bfloat16)


def write_halves(place, result_s, near_ref, far_ref):
    tok_count = near_ref.shape[0]
    half = place & 1
    for which, out_ref in ((half, near_ref), (1 - half, far_ref)):
        at = pl.ds(pl.multiple_of(which * tok_count, tok_count), tok_count)
        out_ref[...] = result_s[at, :]


def far_kernel(
    place_ref, gain_ref, near_keys, far_keys, p2, p3, mixed_b, query_fwd_b, query_bwd_b, fwd_b, bwd_b, end_b, rate_b,
    near_ref, far_ref, value_s, key_s, result_s,
):
    place = place_ref[0]
    arrange_values(place, value_s, p2, p3)
    arrange(place, key_s, near_keys, far_keys)
    keys = key_s[...].astype(jnp.float32)
    rates = [rate_b[at : at + 1, :] for at in range(0, rate_b.shape[0], PACK)]
    scores = scores_of(
        in_blocks(query_fwd_b[...]),
        in_blocks(query_bwd_b[...]),
        in_blocks(keys * fwd_b[...]),
        in_blocks(keys * bwd_b[...]),
        in_blocks(keys * end_b[...]),
        rates,
    )
    mixed = mixed_b[...] + dot_nn(scores, value_s[...])
    result_s[...] = normed_of(mixed, gain_ref[...])
    write_halves(place, result_s, near_ref, far_ref)


def near_kernel(
    place_ref, gain_ref, near_keys, far_keys, p2, p3, mixed_a, query_edge_a, edge_b,
    near_ref, far_ref, value_s, key_s, result_s,
):
    place = place_ref[0]
    arrange_values(place, value_s, p2, p3)
    arrange(place, key_s, near_keys, far_keys)
    key_edge = (key_s[...].astype(jnp.float32) * edge_b[...]).astype(jnp.bfloat16)
    state = dot_tn(key_edge, value_s[...]).astype(jnp.bfloat16)
    mixed = mixed_a[...] + dot_nn(query_edge_a[...], state)
    result_s[...] = normed_of(mixed, gain_ref[...])
    write_halves(place, result_s, near_ref, far_ref)


def on_chip(kernel, place, operands, shapes, scratch):
    return pl.pallas_call(
        kernel,
        in_specs=[pl.BlockSpec(memory_space=pltpu.SMEM)]
        + [pl.BlockSpec(memory_space=pltpu.VMEM)] * len(operands),
        out_specs=[pl.BlockSpec(memory_space=pltpu.VMEM)] * len(shapes),
        out_shape=[jax.ShapeDtypeStruct(*shape) for shape in shapes],
        scratch_shapes=[pltpu.VMEM(*shape) for shape in scratch],
        compiler_params=room(16),
    )(place, *inner(operands))


def mix_heads(place, up, bias, gain, own, got, parcels):
    tok_count = tokens_of(parcels[0])
    size = 2 * tok_count
    narrow, wide = jnp.bfloat16, jnp.float32
    query, value, mixed = ((size, DK), narrow), ((size, DV), narrow), ((size, DV), wide)
    factor = ((size, DK), wide)
    rates = ((size // BLOCK * PACK, DK), wide)
    half = ((tok_count, DV), narrow)
    mixed_a, query_edge_a, state_a = on_chip(
        own_kernel,
        place,
        (up, bias, *own, *parcels[:2]),
        [mixed, query, ((DK, DV), narrow)],
        [query, value, query],
    )
    mixed_b, query_fwd_b, query_bwd_b, fwd_b, bwd_b, end_b, edge_b, rate_b = on_chip(
        other_kernel,
        place,
        (up, bias, state_a, *parcels[2:]),
        [mixed, query, query, factor, factor, factor, factor, rates],
        [query],
    )
    scratch = [value, query, value]
    far = on_chip(
        far_kernel,
        place,
        (gain, *got, *parcels[2:], mixed_b, query_fwd_b, query_bwd_b, fwd_b, bwd_b, end_b, rate_b),
        [half, half],
        scratch,
    )
    near = on_chip(
        near_kernel,
        place,
        (gain, *got, *parcels[2:], mixed_a, query_edge_a, edge_b),
        [half, half],
        scratch,
    )
    return [*near, *far]


def join_kernel(place_ref, *refs):
    out_ref = refs[-1]
    for flip, part in enumerate(refs[:-1]):
        at = pl.multiple_of((place_ref[0] ^ flip) * DV, DV)
        out_ref[:, pl.ds(at, DV)] = part[...]


def join_heads(place, parts):
    return pl.pallas_call(
        join_kernel,
        in_specs=[pl.BlockSpec(memory_space=pltpu.SMEM)]
        + [pl.BlockSpec(memory_space=pltpu.VMEM)] * len(parts),
        out_shape=jax.ShapeDtypeStruct((parts[0].shape[0], VAL), jnp.bfloat16),
        compiler_params=room(8),
        name="join",
    )(place, *parts)


def paired_body(
    hidden, queries, values, key_weight, decay_down, decay_up, decay_bias, span_shift, norm_gain
):
    seq_count, tok_count, model_width = hidden.shape
    dp_size = lax.axis_size("dp")
    place = lax.axis_index("sp").reshape(1)
    rank = lax.axis_index("dp").reshape(1)
    token_rows = hidden.reshape(tok_count, model_width)

    small = (
        decay_down.T,
        span_shift.reshape(1, tok_count),
        decay_up,
        decay_bias.reshape(1, -1),
        norm_gain.reshape(1, -1),
    )
    own_piece, sent_piece, own_rows, up, bias, gain, *parcels = prepare(
        place,
        rank,
        token_rows,
        small,
        key_weight,
        queries.reshape(tok_count, KEY),
        values.reshape(tok_count, VAL),
    )
    peer_rows = exchange(token_rows, "sp", 1)
    parcels = [parcels[0]] + [exchange(parcels[flip], "sp", flip) for flip in range(1, HEADS)]

    def gathered(piece):
        pieces = [piece] * dp_size
        for flip in range(2, dp_size, 2):
            pieces[flip] = exchange(piece, "dp", flip)
        for flip in range(0, dp_size, 2):
            pieces[flip + 1] = exchange(pieces[flip], "dp", 1)
        return pieces

    pieces = gathered(sent_piece)
    got = []
    for rows in (own_rows, peer_rows):
        (sent,) = project_keys(rank, (rows,), pieces)
        got.append(exchange(sent, "sp", 2))
    own = project_keys(rank, (own_rows, peer_rows), gathered(own_piece))
    outs = mix_heads(place, up, bias, gain, own, got, parcels)
    parts = [outs[0]] + [exchange(outs[flip], "sp", flip) for flip in range(1, HEADS)]
    return join_heads(place, parts).reshape(seq_count, tok_count, VAL)


def solution(mesh):
    in_specs = (
        P("dp", "sp", None),
        P("dp", "sp", None),
        P("dp", "sp", None),
        P("dp", None),
        P(),
        P(),
        P(),
        P("dp", "sp"),
        P(),
    )
    out_specs = P("dp", "sp", None)
    paired = mesh.shape["sp"] == HEADS and mesh.shape["dp"] % 2 == 0
    body = paired_body if paired else general_body

    return jax.shard_map(body, mesh=mesh, in_specs=in_specs, out_specs=out_specs, check_vma=False)
```

```python
import jax
import jax.numpy as jnp
from jax import lax
from jax.experimental import pallas as pl
from jax.experimental.pallas import tpu as pltpu

from jax.sharding import PartitionSpec as P

HEADS = 4
DK = 256
DV = 512
BLOCK = 64
KEY = 1024
VAL = 2048


decay_tau = 16.0
norm_eps = 1e-05
highest = lax.Precision.HIGHEST


def mechanism(query, keys_in, value_in, log_decay):
    length, key_width = query.shape
    value_width = value_in.shape[-1]
    blocks = length // BLOCK
    step_decay = log_decay.reshape(blocks, BLOCK, key_width)
    inclusive = jnp.cumsum(step_decay, axis=1)
    exclusive = inclusive - step_decay
    total = inclusive[:, -1, :]
    query3 = query.reshape(blocks, BLOCK, key_width)
    keys3 = keys_in.reshape(blocks, BLOCK, key_width)
    value_tensor3 = value_in.reshape(blocks, BLOCK, value_width)
    query_forward_part = (query3 * jnp.exp(inclusive)).astype(jnp.bfloat16)
    key_fwd = (keys3 * jnp.exp(-inclusive)).astype(jnp.bfloat16)
    query_reverse_part = (query3 * jnp.exp(-exclusive)).astype(jnp.bfloat16)
    key_bwd = (keys3 * jnp.exp(exclusive)).astype(jnp.bfloat16)
    key_end = (keys3 * jnp.exp(total[:, None, :] - inclusive)).astype(jnp.bfloat16)
    fwd_scores = jnp.einsum(
        "nid,njd->nij", query_forward_part, key_fwd, preferred_element_type=jnp.float32
    )
    bwd_scores = jnp.einsum(
        "nid,njd->nij", query_reverse_part, key_bwd, preferred_element_type=jnp.float32
    )
    row_index = lax.broadcasted_iota(jnp.int32, (BLOCK, BLOCK), 0)
    col_index = lax.broadcasted_iota(jnp.int32, (BLOCK, BLOCK), 1)
    attention_scores = jnp.where((col_index <= row_index)[None], fwd_scores, bwd_scores).astype(
        jnp.bfloat16
    )
    inner_block_term = jnp.einsum(
        "ucy,uyh->uch", attention_scores, value_tensor3, preferred_element_type=jnp.float32
    )
    end_terms = jnp.einsum(
        "njd,nje->nde", key_end, value_tensor3, preferred_element_type=jnp.float32
    )
    start_terms = jnp.einsum(
        "njd,nje->nde", key_bwd, value_tensor3, preferred_element_type=jnp.float32
    )
    rates = jnp.exp(total)

    def forward_step(carry_state, inputs):
        rate, term = inputs
        return (rate[:, None] * carry_state + term, carry_state)

    def backward_step(carry_state, inputs):
        rate, term = inputs
        state_here = rate[:, None] * carry_state
        return (state_here + term, state_here)

    empty = jnp.zeros((key_width, value_width), jnp.float32)
    _, forward_scan_states = lax.scan(forward_step, empty, (rates, end_terms))
    _, reverse_scan_states = lax.scan(backward_step, empty, (rates, start_terms), reverse=True)
    produced_rows = jnp.einsum(
        "tzv,tvg->tzg",
        query_forward_part,
        forward_scan_states.astype(jnp.bfloat16),
        preferred_element_type=jnp.float32,
    )
    produced_rows = produced_rows + jnp.einsum(
        "tzv,tvg->tzg",
        query_reverse_part,
        reverse_scan_states.astype(jnp.bfloat16),
        preferred_element_type=jnp.float32,
    )
    return (inner_block_term + produced_rows).reshape(length, value_width).astype(jnp.bfloat16)


def general_body(
    hidden, queries, values, key_weight, decay_down, decay_up, decay_bias, span_shift, norm_gain
):
    seq_count, tok_count, model_width = hidden.shape
    group_size = lax.axis_size("sp")
    value_split = group_size // HEADS
    part_width = DV // value_split
    head_index = lax.axis_index("sp") // value_split
    token_rows = hidden.reshape(tok_count, model_width)

    def per_item(tensor, width):
        by_head = tensor.reshape(tok_count, HEADS, width).transpose(1, 0, 2)
        spread_out = jnp.broadcast_to(by_head[:, None], (HEADS, value_split, tok_count, width))
        return spread_out.reshape(group_size, tok_count, width)

    def every_item(tensor):
        return jnp.broadcast_to(tensor[None], (group_size,) + tensor.shape)

    key_sums = jnp.dot(
        token_rows,
        lax.all_gather(key_weight, "dp", axis=0, tiled=True),
        preferred_element_type=jnp.float32,
    )
    keys = key_sums.astype(jnp.bfloat16)
    head_key = lax.all_to_all(per_item(keys, DK), "sp", split_axis=0, concat_axis=1, tiled=True)[0]
    low = jnp.dot(token_rows, decay_down, preferred_element_type=jnp.float32).astype(jnp.bfloat16)
    value_items = values.reshape(tok_count, group_size, part_width).transpose(1, 0, 2)
    head_query, head_value, head_low, head_shift = (
        lax.all_to_all(
            per_item(queries.reshape(tok_count, KEY), DK),
            "sp",
            split_axis=0,
            concat_axis=1,
            tiled=True,
        ),
        lax.all_to_all(value_items, "sp", split_axis=0, concat_axis=1, tiled=True),
        lax.all_to_all(every_item(low), "sp", split_axis=0, concat_axis=1, tiled=True),
        lax.all_to_all(
            every_item(span_shift.reshape(tok_count, 1)),
            "sp",
            split_axis=0,
            concat_axis=1,
            tiled=True,
        ),
    )
    up_columns = lax.dynamic_slice_in_dim(decay_up, head_index * DK, DK, 1)
    bias_part = lax.dynamic_slice_in_dim(decay_bias, head_index * DK, DK, 0)
    pre = jnp.dot(
        head_low[0].astype(jnp.float32),
        up_columns,
        precision=highest,
        preferred_element_type=jnp.float32,
    )
    pre = pre + bias_part[None, :] + head_shift[0].astype(jnp.float32)
    log_decay = jax.nn.log_sigmoid(pre) / decay_tau
    scaled = head_query[0].astype(jnp.float32) * DK ** (-0.5)
    mixed = mechanism(scaled, head_key.astype(jnp.float32), head_value[0], log_decay)
    returned = lax.all_to_all(mixed[None], "sp", split_axis=1, concat_axis=0, tiled=True)
    grouped = returned.astype(jnp.float32).transpose(1, 0, 2).reshape(tok_count, HEADS, DV)
    normed = grouped * lax.rsqrt(jnp.mean(grouped * grouped, axis=-1, keepdims=True) + norm_eps)
    normed = normed * norm_gain.reshape(HEADS, DV)[None]
    return normed.reshape(seq_count, tok_count, VAL).astype(jnp.bfloat16)


PACK = 8


def room(mebibytes):
    return pltpu.CompilerParams(vmem_limit_bytes=mebibytes * 2**20)


def inner(tensors):
    return [pltpu.with_memory_space_constraint(tensor, pltpu.VMEM) for tensor in tensors]


def exchange(tensor, axis, flip):
    size = lax.axis_size(axis)
    return lax.ppermute(tensor, axis, [(i, i ^ flip) for i in range(size)])


def dot_nn(left, right):
    return lax.dot_general(
        left, right, (((1,), (0,)), ((), ())), preferred_element_type=jnp.float32
    )


def dot_nt(left, right):
    return lax.dot_general(
        left, right, (((1,), (1,)), ((), ())), preferred_element_type=jnp.float32
    )


def dot_tn(left, right):
    return lax.dot_general(
        left, right, (((0,), (0,)), ((), ())), preferred_element_type=jnp.float32
    )


def prepare_kernel(
    place_ref, rank_ref, down_ref, shift_ref, up_ref, bias_ref, gain_ref, weight_ref, hidden_ref, query_ref,
    value_ref, own_piece, sent_piece, hidden_out, up_out, bias_out, gain_out, p0, p1, p2, p3, down_s, shift_s, sems,
):
    parcels = (p0, p1, p2, p3)
    place = place_ref[0]
    tok_count = query_ref.shape[0]
    copies = []

    def fetch(source, target, head=None, width=None):
        if width is not None:
            source = source.at[:, pl.ds(pl.multiple_of(head * width, width), width)]
        copies.append(pltpu.make_async_copy(source, target, sems.at[len(copies)]))
        copies[-1].start()

    fetch(hidden_ref, hidden_out)
    fetch(down_ref, down_s)
    fetch(shift_ref, shift_s)
    fetch(weight_ref, sent_piece, place ^ 2, DK)
    fetch(weight_ref, own_piece, place, DK)
    for flip in (2, 3, 1, 0):
        head = place ^ flip
        sources = ((query_ref, head), (value_ref, 2 * head), (value_ref, 2 * head + 1))
        for slot, (source, column) in enumerate(sources):
            rows = parcels[flip].at[pl.ds(slot * tok_count, tok_count), :]
            fetch(source, rows, column, DK)
    fetch(up_ref, up_out, place, DK)
    fetch(bias_ref, bias_out, place, DK)
    fetch(gain_ref, gain_out, place, DV)
    for copy in copies[:3]:
        copy.wait()
    low = dot_nt(down_s[...], hidden_out[...]).astype(jnp.bfloat16).astype(jnp.float32)
    shift = jnp.broadcast_to(shift_s[...].astype(jnp.float32), (PACK, tok_count))
    low = jnp.concatenate([low[:PACK], low[PACK:]], axis=1)
    shift = jnp.concatenate([shift, shift], axis=1)
    tail = jnp.concatenate([low, shift], axis=0).astype(jnp.bfloat16)
    for parcel in parcels:
        parcel[3 * tok_count :, :] = tail
    for copy in copies[3:]:
        copy.wait()


def prepare(place, rank, token_rows, small, key_weight, queries, values):
    tok_count, rows = token_rows.shape[0], key_weight.shape[0]
    down, shift, up, bias, gain = small
    outer = [
        pltpu.with_memory_space_constraint(a, pltpu.HBM)
        for a in (down, shift, up, bias, gain, key_weight, token_rows, queries, values)
    ]
    parcel = jax.ShapeDtypeStruct((3 * tok_count + 2 * PACK, DK), jnp.bfloat16)
    shapes = [
        jax.ShapeDtypeStruct((rows, DK), jnp.bfloat16),
        jax.ShapeDtypeStruct((rows, DK), jnp.bfloat16),
        jax.ShapeDtypeStruct(token_rows.shape, jnp.bfloat16),
        jax.ShapeDtypeStruct((up.shape[0], DK), jnp.float32),
        jax.ShapeDtypeStruct((1, DK), jnp.float32),
        jax.ShapeDtypeStruct((1, DV), jnp.float32),
    ]
    return pl.pallas_call(
        prepare_kernel,
        in_specs=[pl.BlockSpec(memory_space=pltpu.SMEM)] * 2
        + [pl.BlockSpec(memory_space=pl.ANY)] * len(outer),
        out_specs=[pl.BlockSpec(memory_space=pltpu.VMEM)] * (len(shapes) + HEADS),
        out_shape=[pltpu.VMEM(a.shape, a.dtype) for a in shapes + [parcel] * HEADS],
        scratch_shapes=[
            pltpu.VMEM(down.shape, down.dtype),
            pltpu.VMEM(shift.shape, shift.dtype),
            pltpu.SemaphoreType.DMA((8 + 3 * HEADS,)),
        ],
        compiler_params=room(8),
        name="prepare",
    )(place, rank, *outer)


def keys_kernel(rank_ref, *refs):
    count = lax.axis_size("dp")
    sets = (len(refs) - count) // 2
    pieces = refs[sets : sets + count]
    for tokens, keys in zip(refs[:sets], refs[sets + count :]):
        sums = jnp.zeros(keys.shape, jnp.float32)
        for flip, piece in enumerate(pieces):
            rows = piece.shape[0]
            at = pl.multiple_of((rank_ref[0] ^ flip) * rows, rows)
            sums = sums + dot_nn(tokens[:, pl.ds(at, rows)], piece[...])
        keys[...] = sums.astype(jnp.bfloat16)


def project_keys(rank, tokens, pieces):
    operands = (*tokens, *pieces)
    return pl.pallas_call(
        keys_kernel,
        in_specs=[pl.BlockSpec(memory_space=pltpu.SMEM)]
        + [pl.BlockSpec(memory_space=pltpu.VMEM)] * len(operands),
        out_shape=[jax.ShapeDtypeStruct((rows.shape[0], DK), jnp.bfloat16) for rows in tokens],
        compiler_params=room(12),
        name="keys",
    )(rank, *inner(operands))


def split3(tensor):
    first = tensor.astype(jnp.bfloat16)
    rest = tensor - first.astype(jnp.float32)
    second = rest.astype(jnp.bfloat16)
    third = (rest - second.astype(jnp.float32)).astype(jnp.bfloat16)
    return first, second, third


def in_blocks(tensor):
    return [tensor[at : at + BLOCK] for at in range(0, tensor.shape[0], BLOCK)]


def arrange(place, target, near, far):
    tok_count = target.shape[0] // 2
    half = place & 1
    for which, part in ((half, near), (1 - half, far)):
        at = pl.ds(pl.multiple_of(which * tok_count, tok_count), tok_count)
        target[at, :] = part[...]


def tokens_of(parcel):
    return (parcel.shape[0] - 2 * PACK) // 3


def query_of(parcel):
    return parcel.at[: tokens_of(parcel), :]


def arrange_values(place, target, near, far):
    tok_count = target.shape[0] // 2
    half = place & 1
    for which, part in ((half, near), (1 - half, far)):
        at = pl.ds(pl.multiple_of(which * tok_count, tok_count), tok_count)
        target[at, :DK] = part[tok_count : 2 * tok_count, :]
        target[at, DK:] = part[2 * tok_count : 3 * tok_count, :]


def arrange_low(place, near, far):
    tok_count = tokens_of(near)
    near, far = (part[3 * tok_count :, :].astype(jnp.float32) for part in (near, far))
    odd = (place & 1) == 1
    halves = []
    for part in (jnp.where(odd, far, near), jnp.where(odd, near, far)):
        low = [part[:PACK, :tok_count], part[:PACK, tok_count:]]
        shift = part[PACK:, :tok_count]
        row = lax.broadcasted_iota(jnp.int32, shift.shape, 0)
        first = jnp.where(row == 0, shift, 0.0)
        halves.append(jnp.concatenate(low * 3 + [first, jnp.zeros_like(first)], axis=0))
    return jnp.concatenate(halves, axis=1).astype(jnp.bfloat16)


def decay_of(low, up, bias, sum_up_to):
    pre = dot_tn(low, up) + bias
    decay = (jnp.minimum(pre, 0.0) - jnp.log1p(jnp.exp(-jnp.abs(pre)))) * (1.0 / decay_tau)
    inclusive = sum(dot_nn(sum_up_to, part) for part in split3(decay))
    return decay, inclusive


def scores_of(query_fwd, query_bwd, key_fwd, key_bwd, key_end, rates):
    blocks = len(rates)
    short = lambda tensors: [tensor.astype(jnp.bfloat16) for tensor in tensors]
    key_fwd, near_bwd = short(key_fwd), short(key_bwd)
    width = blocks * BLOCK
    row = lax.broadcasted_iota(jnp.int32, (BLOCK, width), 0)
    col = lax.broadcasted_iota(jnp.int32, (BLOCK, width), 1)
    rows = []
    for here in range(blocks):
        left, right = list(key_fwd), list(near_bwd)
        for past in range(here):
            faded = key_end[past]
            for between in range(past + 1, here):
                faded = faded * rates[between]
            left[past] = faded.astype(jnp.bfloat16)
        fade = None
        for later in range(here + 1, blocks):
            fade = rates[later - 1] if fade is None else fade * rates[later - 1]
            right[later] = (key_bwd[later] * fade).astype(jnp.bfloat16)
        fwd = dot_nt(query_fwd[here], jnp.concatenate(left, axis=0))
        bwd = dot_nt(query_bwd[here], jnp.concatenate(right, axis=0))
        rows.append(jnp.where(col <= row + here * BLOCK, fwd, bwd).astype(jnp.bfloat16))
    return jnp.concatenate(rows, axis=0)


def factors(decay, inclusive, facing_right):
    blocks = zip(in_blocks(decay), in_blocks(inclusive))
    decay, inclusive = map(list, zip(*blocks))
    totals = [tensor[BLOCK - 1 :] for tensor in inclusive]
    none = jnp.zeros_like(totals[0])
    right = jnp.where(facing_right, 1.0, 0.0)
    found = []
    for at in range(len(totals)):
        exclusive = inclusive[at] - decay[at]
        before = sum(totals[:at], none)
        after = sum(totals[at:], none)
        base = right * after + (1.0 - right) * before
        sign = 1.0 - 2.0 * right
        found.append(
            dict(
                query_fwd=jnp.exp(inclusive[at]),
                query_bwd=jnp.exp(-exclusive),
                key_fwd=jnp.exp(-inclusive[at]),
                key_bwd=jnp.exp(exclusive),
                key_end=jnp.exp(totals[at] - inclusive[at]),
                key_edge=jnp.exp(base + sign * (exclusive + right * decay[at])),
                query_edge=jnp.exp(base + sign * (inclusive[at] - right * decay[at])),
                rate=jnp.exp(totals[at]),
            )
        )
    return {name: [one[name] for one in found] for name in found[0]}


def decay_inputs(up_ref, bias_ref, size):
    rank = up_ref.shape[0]
    ones = (lax.broadcasted_iota(jnp.int32, (rank, DK), 0) == 0).astype(jnp.float32)
    up = jnp.concatenate(
        [part.astype(jnp.float32) for part in split3(up_ref[...])] + [ones], axis=0
    ).astype(jnp.bfloat16)
    row = lax.broadcasted_iota(jnp.int32, (size, size), 0)
    col = lax.broadcasted_iota(jnp.int32, (size, size), 1)
    lower = ((row // BLOCK) == (col // BLOCK)) & (col <= row)
    return up, bias_ref[...], jnp.where(lower, 1.0, 0.0).astype(jnp.bfloat16)


def joined(tensors):
    return jnp.concatenate(tensors, axis=0)


def times(left, right):
    return [a * b for a, b in zip(left, right)]


def short(tensors):
    return [tensor.astype(jnp.bfloat16) for tensor in tensors]


def own_kernel(
    place_ref, up_ref, bias_ref, near_keys, far_keys, p0, p1, query_edge_b,
    mixed_a, mixed_b, query_edge_a, query_s, value_s, key_s,
):
    place = place_ref[0]
    size = mixed_a.shape[0]
    arrange(place, query_s, query_of(p0), query_of(p1))
    arrange_values(place, value_s, p0, p1)
    arrange(place, key_s, near_keys, far_keys)
    up, bias, sum_up_to = decay_inputs(up_ref, bias_ref, size)
    low = arrange_low(place, p0, p1)
    found = factors(*decay_of(low, up, bias, sum_up_to), place < HEADS // 2)
    scaled = in_blocks(query_s[...].astype(jnp.float32) * DK**-0.5)
    keys = in_blocks(key_s[...].astype(jnp.float32))
    scores = scores_of(
        short(times(scaled, found["query_fwd"])),
        short(times(scaled, found["query_bwd"])),
        times(keys, found["key_fwd"]),
        times(keys, found["key_bwd"]),
        times(keys, found["key_end"]),
        found["rate"],
    )
    mixed_a[...] = dot_nn(scores, value_s[...])
    query_edge_a[...] = joined(short(times(scaled, found["query_edge"])))
    key_edge = joined(short(times(keys, found["key_edge"])))
    state = dot_tn(key_edge, value_s[...]).astype(jnp.bfloat16)
    mixed_b[...] = dot_nn(query_edge_b[...], state)


def other_kernel(
    place_ref, up_ref, bias_ref, own_keys, p2, p3,
    query_edge_b, value_b, query_fwd_b, query_bwd_b, fwd_b, bwd_b, end_b, edge_b, rate_b, query_s,
):
    place = place_ref[0]
    arrange(place, query_s, query_of(p2), query_of(p3))
    arrange_values(place, value_b, p2, p3)
    up, bias, sum_up_to = decay_inputs(up_ref, bias_ref, query_s.shape[0])
    low = arrange_low(place, p2, p3)
    found = factors(*decay_of(low, up, bias, sum_up_to), place >= HEADS // 2)
    scaled = in_blocks(query_s[...].astype(jnp.float32) * DK**-0.5)
    query_fwd_b[...] = joined(short(times(scaled, found["query_fwd"])))
    query_bwd_b[...] = joined(short(times(scaled, found["query_bwd"])))
    query_edge_b[...] = joined(short(times(scaled, found["query_edge"])))
    fwd_b[...] = joined(found["key_fwd"])
    bwd_b[...] = joined(found["key_bwd"])
    end_b[...] = joined(found["key_end"])
    edge_b[...] = joined(found["key_edge"])
    for at, rate in enumerate(found["rate"]):
        rate_b[at * PACK : (at + 1) * PACK, :] = jnp.broadcast_to(rate, (PACK, DK))


def normed_of(mixed, gain):
    mixed = mixed.astype(jnp.bfloat16).astype(jnp.float32)
    mean = jnp.mean(mixed * mixed, axis=-1, keepdims=True)
    return mixed * lax.rsqrt(mean + norm_eps) * gain


def in_order(place, near, far):
    odd = (place & 1) == 1
    return jnp.where(odd, far, near), jnp.where(odd, near, far)


def ordered_keys(place, near_keys, far_keys):
    halves = (keys[...].astype(jnp.float32) for keys in (near_keys, far_keys))
    return joined(in_order(place, *halves))


def write_halves(place, result, near_ref, far_ref):
    tok_count = near_ref.shape[0]
    near, far = in_order(place, result[:tok_count], result[tok_count:])
    near_ref[...] = near.astype(jnp.bfloat16)
    far_ref[...] = far.astype(jnp.bfloat16)


def far_kernel(
    place_ref, gain_ref, near_keys, far_keys, value_b, mixed_b, query_fwd_b, query_bwd_b, fwd_b, bwd_b,
    end_b, rate_b, near_ref, far_ref,
):
    place = place_ref[0]
    keys = ordered_keys(place, near_keys, far_keys)
    rates = [rate_b[at : at + 1, :] for at in range(0, rate_b.shape[0], PACK)]
    scores = scores_of(
        in_blocks(query_fwd_b[...]),
        in_blocks(query_bwd_b[...]),
        in_blocks(keys * fwd_b[...]),
        in_blocks(keys * bwd_b[...]),
        in_blocks(keys * end_b[...]),
        rates,
    )
    mixed = mixed_b[...] + dot_nn(scores, value_b[...])
    write_halves(place, normed_of(mixed, gain_ref[...]), near_ref, far_ref)


def near_kernel(
    place_ref, gain_ref, near_keys, far_keys, value_b, mixed_a, query_edge_a, edge_b, near_ref, far_ref
):
    place = place_ref[0]
    keys = ordered_keys(place, near_keys, far_keys)
    state = dot_tn((keys * edge_b[...]).astype(jnp.bfloat16), value_b[...]).astype(jnp.bfloat16)
    mixed = mixed_a[...] + dot_nn(query_edge_a[...], state)
    write_halves(place, normed_of(mixed, gain_ref[...]), near_ref, far_ref)


def on_chip(kernel, place, operands, shapes, scratch):
    return pl.pallas_call(
        kernel,
        in_specs=[pl.BlockSpec(memory_space=pltpu.SMEM)]
        + [pl.BlockSpec(memory_space=pltpu.VMEM)] * len(operands),
        out_specs=[pl.BlockSpec(memory_space=pltpu.VMEM)] * len(shapes),
        out_shape=[jax.ShapeDtypeStruct(*shape) for shape in shapes],
        scratch_shapes=[pltpu.VMEM(*shape) for shape in scratch],
        compiler_params=room(16),
    )(place, *inner(operands))


def mix_heads(place, up, bias, gain, own, got, parcels):
    tok_count = tokens_of(parcels[0])
    size = 2 * tok_count
    narrow, wide = jnp.bfloat16, jnp.float32
    query, value, mixed = ((size, DK), narrow), ((size, DV), narrow), ((size, DV), wide)
    factor = ((size, DK), wide)
    rates = ((size // BLOCK * PACK, DK), wide)
    half = ((tok_count, DV), narrow)
    query_edge_b, value_b, query_fwd_b, query_bwd_b, fwd_b, bwd_b, end_b, edge_b, rate_b = on_chip(
        other_kernel,
        place,
        (up, bias, own[0], *parcels[2:]),
        [query, value, query, query, factor, factor, factor, factor, rates],
        [query],
    )
    mixed_a, mixed_b, query_edge_a = on_chip(
        own_kernel,
        place,
        (up, bias, *own, *parcels[:2], query_edge_b),
        [mixed, mixed, query],
        [query, value, query],
    )
    far = on_chip(
        far_kernel,
        place,
        (gain, *got, value_b, mixed_b, query_fwd_b, query_bwd_b, fwd_b, bwd_b, end_b, rate_b),
        [half, half],
        [],
    )
    near = on_chip(
        near_kernel, place, (gain, *got, value_b, mixed_a, query_edge_a, edge_b), [half, half], []
    )
    return [*near, *far]


def join_kernel(place_ref, *refs):
    out_ref = refs[-1]
    for flip, part in enumerate(refs[:-1]):
        at = pl.multiple_of((place_ref[0] ^ flip) * DV, DV)
        out_ref[:, pl.ds(at, DV)] = part[...]


def join_heads(place, parts):
    return pl.pallas_call(
        join_kernel,
        in_specs=[pl.BlockSpec(memory_space=pltpu.SMEM)]
        + [pl.BlockSpec(memory_space=pltpu.VMEM)] * len(parts),
        out_shape=jax.ShapeDtypeStruct((parts[0].shape[0], VAL), jnp.bfloat16),
        compiler_params=room(8),
        name="join",
    )(place, *parts)


def paired_body(
    hidden, queries, values, key_weight, decay_down, decay_up, decay_bias, span_shift, norm_gain
):
    seq_count, tok_count, model_width = hidden.shape
    dp_size = lax.axis_size("dp")
    place = lax.axis_index("sp").reshape(1)
    rank = lax.axis_index("dp").reshape(1)
    token_rows = hidden.reshape(tok_count, model_width)

    small = (
        decay_down.T,
        span_shift.reshape(1, tok_count),
        decay_up,
        decay_bias.reshape(1, -1),
        norm_gain.reshape(1, -1),
    )
    own_piece, sent_piece, own_rows, up, bias, gain, *parcels = prepare(
        place,
        rank,
        token_rows,
        small,
        key_weight,
        queries.reshape(tok_count, KEY),
        values.reshape(tok_count, VAL),
    )
    peer_rows = exchange(token_rows, "sp", 1)
    parcels = [parcels[0]] + [exchange(parcels[flip], "sp", flip) for flip in range(1, HEADS)]

    def gathered(piece):
        pieces = [piece] * dp_size
        for flip in range(2, dp_size, 2):
            pieces[flip] = exchange(piece, "dp", flip)
        for flip in range(0, dp_size, 2):
            pieces[flip + 1] = exchange(pieces[flip], "dp", 1)
        return pieces

    pieces = gathered(sent_piece)
    got = []
    for rows in (own_rows, peer_rows):
        (sent,) = project_keys(rank, (rows,), pieces)
        got.append(exchange(sent, "sp", 2))
    own = project_keys(rank, (own_rows, peer_rows), gathered(own_piece))
    outs = mix_heads(place, up, bias, gain, own, got, parcels)
    parts = [outs[0]] + [exchange(outs[flip], "sp", flip) for flip in range(1, HEADS)]
    return join_heads(place, parts).reshape(seq_count, tok_count, VAL)


def solution(mesh):
    in_specs = (
        P("dp", "sp", None),
        P("dp", "sp", None),
        P("dp", "sp", None),
        P("dp", None),
        P(),
        P(),
        P(),
        P("dp", "sp"),
        P(),
    )
    out_specs = P("dp", "sp", None)
    paired = mesh.shape["sp"] == HEADS and mesh.shape["dp"] % 2 == 0
    body = paired_body if paired else general_body

    return jax.shard_map(body, mesh=mesh, in_specs=in_specs, out_specs=out_specs, check_vma=False)
```
